32 devices in a mesh: sp: 4 (over z), fs: 4 (over y, x), tp: 2 (over core).
Axes of the slice: x: 2, y: 2, z: 4, core: 2. Of those that a mesh axis runs over, the one named last changes fastest.
Arguments:
- tokens: bfloat16 [4, 512, 2048], P('fs', ('sp', 'tp')), may hold values from -6 to 6
- norm_gain: float32 [2048], replicated, may hold values from 0.1 to 1.9
- rec_query: bfloat16 [2048, 512], P('sp', 'tp'), may hold values from -0.125 to 0.125
- rec_input: bfloat16 [2048, 512], P('sp', 'tp'), may hold values from -0.125 to 0.125
- rec_forward: bfloat16 [2048, 512], P('sp', 'tp'), may hold values from -0.125 to 0.125
- rec_backward: bfloat16 [2048, 512], P('sp', 'tp'), may hold values from -0.125 to 0.125
- forget_gap: float32 [2, 512], P(None, 'tp'), may hold values from 0 to 0.06
- log_decay: float32 [4, 2, 4, 512], P('fs', None, 'tp', 'sp'), may hold values from -0.7 to 0
- rec_gain: float32 [512], P('tp'), may hold values from 0.1 to 1.9
- conv_value: bfloat16 [2048, 512], P('sp', 'tp'), may hold values from -0.125 to 0.125
- conv_gate: bfloat16 [2048, 512], P('sp', 'tp'), may hold values from -0.125 to 0.125
- conv_kernel: bfloat16 [31, 512], P(None, 'tp'), may hold values from -3.1 to 3.1
- conv_gain: float32 [512], P('tp'), may hold values from 0.1 to 1.9
- out_rec: bfloat16 [512, 2048], P('tp', 'sp'), may hold values from -0.1875 to 0.1875
- out_conv: bfloat16 [512, 2048], P('tp', 'sp'), may hold values from -0.1875 to 0.1875
Outputs:
- mixed: bfloat16 [4, 512, 2048], P('fs', ('sp', 'tp'))
The draws below stay inside these ranges and needn't reach their ends.
All inputs are finite; a program needn't handle non-finite values.
Results may differ from the reference program's by a relative error of at most 0.017.
Values may be sent and summed in bfloat16 or wider, within the bound.
A program may use at most 64 MiB of HBM per device.

```python
import jax
import jax.numpy as jnp
from jax import lax

D = 2048
RECURRENCE_HEADS = 4
KD = 128
VD = 128
CONV_WIDTH = 31
BLOCK = 64
TOK_DEV = 128
SEQUENCE_LENGTH = 512
SEQUENCE_COUNT = 4
GW = 512
KW = 512


def draw_forget_gap(key, part):
    rng_fast = jax.random.fold_in(key, 11)
    rng_gap = jax.random.fold_in(key, 12)
    fast_heads = jax.random.randint(rng_fast, (2, RECURRENCE_HEADS, 1), 0, 2) == 0
    spread = jax.random.uniform(rng_gap, (2, RECURRENCE_HEADS, KD), jnp.float32)
    fast_gap = 0.02 * jnp.power(3.0, spread)
    slow_gap = 0.2 * jnp.power(5.0, spread) / SEQUENCE_LENGTH
    chosen = jnp.where(fast_heads, fast_gap, slow_gap)
    return chosen.reshape(2, RECURRENCE_HEADS * KD).astype(jnp.float32)


def draw_log_decay(key, part):
    rng_rate = jax.random.fold_in(key, 21)
    random_spike_key = jax.random.fold_in(key, 22)
    random_length_key = jax.random.fold_in(key, 23)
    segments = SEQUENCE_LENGTH // TOK_DEV
    spread = jax.random.uniform(rng_rate, (SEQUENCE_COUNT, 2, RECURRENCE_HEADS, segments, 1), jnp.float32)
    spike_probability = 0.1 * jnp.power(10.0, spread) / SEQUENCE_LENGTH
    spike_probability = jnp.broadcast_to(spike_probability, (SEQUENCE_COUNT, 2, RECURRENCE_HEADS, segments, TOK_DEV)).reshape(SEQUENCE_COUNT, 2, RECURRENCE_HEADS, SEQUENCE_LENGTH)
    spike_active = jax.random.randint(random_spike_key, (SEQUENCE_COUNT, 2, RECURRENCE_HEADS, SEQUENCE_LENGTH), 0, SEQUENCE_LENGTH) < 2
    spike_length = jax.random.uniform(random_length_key, (SEQUENCE_COUNT, 2, RECURRENCE_HEADS, SEQUENCE_LENGTH), jnp.float32, 0.22, 0.69)
    return -(spike_probability + jnp.where(spike_active, spike_length, 0.0)).astype(jnp.float32)


def draw_conv_kernel(key, part):
    rng_base = jax.random.fold_in(key, 31)
    rng_scale = jax.random.fold_in(key, 32)
    channel_pos = jnp.arange(GW, dtype=jnp.float32) / max(GW - 1, 1)
    wobble = jax.random.uniform(rng_scale, (GW,), jnp.float32, jnp.log(0.7), jnp.log(1.4))
    channel_scale = jnp.exp(jnp.log(3.0) * channel_pos + wobble)
    base_draw = jnp.clip(jax.random.normal(rng_base, (CONV_WIDTH, GW), jnp.float32), -4.0, 4.0)
    return (base_draw * channel_scale[None, :] / jnp.sqrt(CONV_WIDTH * 1.0)).astype(jnp.bfloat16)


def block_levels(own_key, shape, split, least, largest):
    def one(dim, blocks):
        steps = jax.random.uniform(jax.random.fold_in(jax.random.fold_in(own_key, 6), dim), (blocks,), jnp.float32, least / len(split), largest / len(split))
        return jnp.repeat(jnp.exp(steps), shape[dim] // blocks).reshape((-1,) + (1,) * (len(shape) - dim - 1))

    gain = one(*split[0])
    for cut in split[1:]:
        gain = gain * one(*cut)
    return gain


def scatter_about(stream_key, dims, deviation, limit, cuts=(), kind=jnp.bfloat16):
    drawn = jax.random.normal(stream_key, dims, jnp.float32) * deviation
    if len(cuts) > 0:
        drawn = block_levels(stream_key, dims, cuts, -0.22, 0.18) * drawn
    return jnp.clip(drawn, min=-limit, max=limit).astype(kind)


def setup_inputs(seed: int = 0) -> dict:
    splits = jax.random.split(jax.random.key(seed), 16)
    return {
        "tokens": scatter_about(splits[0], (SEQUENCE_COUNT, SEQUENCE_LENGTH, D), 1.0, 6.0, ((0, 4), (1, 8))),
        "norm_gain": jnp.clip(1.0 + 0.18 * jax.random.normal(splits[1], (D,), jnp.float32), 0.1, 1.9),
        "rec_query": scatter_about(splits[2], (D, KW), D ** -0.5, 0.125, ((0, 4), (1, 2))),
        "rec_input": scatter_about(splits[3], (D, GW), D ** -0.5, 0.125, ((0, 4), (1, 2))),
        "rec_forward": scatter_about(splits[4], (D, KW), D ** -0.5, 0.125, ((0, 4), (1, 2))),
        "rec_backward": scatter_about(splits[5], (D, KW), D ** -0.5, 0.125, ((0, 4), (1, 2))),
        "forget_gap": draw_forget_gap(jax.random.fold_in(splits[15], 71), 0),
        "log_decay": draw_log_decay(jax.random.fold_in(splits[15], 71), 0),
        "rec_gain": jnp.clip(1.0 + 0.18 * jax.random.normal(splits[8], (GW,), jnp.float32), 0.1, 1.9),
        "conv_value": scatter_about(splits[9], (D, GW), D ** -0.5, 0.125, ((0, 4), (1, 2))),
        "conv_gate": scatter_about(splits[10], (D, GW), D ** -0.5, 0.125, ((0, 4), (1, 2))),
        "conv_kernel": draw_conv_kernel(jax.random.fold_in(splits[15], 71), 0),
        "conv_gain": jnp.clip(1.0 + 0.18 * jax.random.normal(splits[12], (GW,), jnp.float32), 0.1, 1.9),
        "out_rec": scatter_about(splits[13], (GW, D), (2 * GW) ** -0.5, 0.1875, ((0, 2), (1, 4))),
        "out_conv": scatter_about(splits[14], (GW, D), (2 * GW) ** -0.5, 0.1875, ((0, 2), (1, 4))),
    }


EPS = 1e-06
HIGH = lax.Precision.HIGHEST

def block_scan(queries, key_rows, value_rows, log_gate):
    heads_n, length_n, key_dim = queries.shape
    value_dim = value_rows.shape[-1]
    blocks = length_n // BLOCK

    def split_blocks(tensor):
        return tensor.reshape(heads_n, blocks, BLOCK, tensor.shape[-1]).transpose(1, 0, 2, 3)
    lower_mask = jnp.tril(jnp.ones((BLOCK, BLOCK), bool))

    def advance(states, inputs):
        query_b, key_b, value_b, gate_b = inputs
        cumulative = jnp.cumsum(gate_b, axis=1)
        query_g = query_b * jnp.exp(cumulative)
        key_g = key_b * jnp.exp(-cumulative)
        scores = jnp.einsum('htd,hsd->hts', query_g, key_g, precision=HIGH)
        scores = jnp.where(lower_mask, scores, 0.0)
        result = jnp.einsum('hts,hse->hte', scores, value_b, precision=HIGH)
        result = result + jnp.einsum('htd,hde->hte', query_g, states, precision=HIGH)
        last_g = cumulative[:, -1, :]
        weighted = key_b * jnp.exp(last_g[:, None, :] - cumulative)
        states = jnp.exp(last_g)[:, :, None] * states + jnp.einsum('hsd,hse->hde', weighted, value_b, precision=HIGH)
        return (states, result)
    start_state = jnp.zeros((heads_n, key_dim, value_dim), jnp.float32)
    inputs = (split_blocks(queries), split_blocks(key_rows), split_blocks(value_rows), split_blocks(log_gate))
    final_state, results = lax.scan(advance, start_state, inputs)
    return results.transpose(1, 0, 2, 3).reshape(heads_n, length_n, value_dim)

def to_heads(tensor):
    return tensor.astype(jnp.float32).reshape(tensor.shape[0], RECURRENCE_HEADS, -1).transpose(1, 0, 2)

def gate_terms(pre_act, gap_row, decay_row):
    closing = jax.nn.sigmoid(-to_heads(pre_act)) * gap_row.reshape(RECURRENCE_HEADS, 1, -1)
    return (closing, jnp.log1p(-closing) + decay_row[:, :, None])

def reference(tokens, norm_gain, rec_query, rec_input, rec_forward, rec_backward, forget_gap, log_decay, rec_gain, conv_value, conv_gate, conv_kernel, conv_gain, out_rec, out_conv):

    def one_sequence(inputs):
        rows_in, decay_in = inputs
        row_values = rows_in.astype(jnp.float32)
        normed = row_values * lax.rsqrt(lax.optimization_barrier(jnp.mean(row_values * row_values, axis=-1, keepdims=True)) + EPS)
        normed = (normed * norm_gain).astype(jnp.bfloat16)

        def project(weight):
            return jnp.dot(normed, weight, preferred_element_type=jnp.float32).astype(jnp.bfloat16)
        queries = jax.nn.silu(to_heads(project(rec_query))) * KD ** (-0.5)
        values = to_heads(project(rec_input))
        keys_fwd, gate_fwd = gate_terms(project(rec_forward), forget_gap[0], decay_in[0])
        keys_bwd, gate_bwd = gate_terms(project(rec_backward), forget_gap[1], decay_in[1])
        forward = block_scan(queries, keys_fwd, values, gate_fwd)
        backward = jnp.flip(block_scan(jnp.flip(queries, 1), jnp.flip(keys_bwd, 1), jnp.flip(values, 1), jnp.flip(gate_bwd, 1)), 1)
        joined = forward + backward
        joined = joined * lax.rsqrt(lax.optimization_barrier(jnp.mean(joined * joined, axis=-1, keepdims=True)) + EPS)
        joined = joined * rec_gain.reshape(RECURRENCE_HEADS, 1, VD)
        rec_out = joined.transpose(1, 0, 2).reshape(SEQUENCE_LENGTH, GW).astype(jnp.bfloat16)
        conv_pre = project(conv_value).astype(jnp.float32)
        glu_pre = project(conv_gate).astype(jnp.float32)
        gated = (conv_pre * jax.nn.sigmoid(glu_pre)).astype(jnp.bfloat16)
        convolved = lax.conv_general_dilated(gated.astype(jnp.float32)[None], conv_kernel.astype(jnp.float32)[:, None, :], (1,), 'SAME', dimension_numbers=('NWC', 'WIO', 'NWC'), feature_group_count=GW, precision=HIGH)[0]
        mean_c = lax.optimization_barrier(jnp.sum(convolved, axis=-1, keepdims=True)) / GW
        variance = lax.optimization_barrier(jnp.sum(convolved * convolved, axis=-1, keepdims=True)) / GW - mean_c * mean_c
        conv_out = jax.nn.silu((convolved - mean_c) * lax.rsqrt(variance + EPS) * conv_gain).astype(jnp.bfloat16)
        mixed = jnp.dot(rec_out, out_rec, preferred_element_type=jnp.float32)
        mixed = mixed + jnp.dot(conv_out, out_conv, preferred_element_type=jnp.float32)
        return mixed.astype(jnp.bfloat16)
    return lax.map(one_sequence, (tokens, log_decay))
```

```python
import functools

import jax
import jax.numpy as jnp
from jax import lax
from jax.experimental import pallas as pl
from jax.experimental.pallas import tpu as pltpu
from jax.sharding import PartitionSpec as P

KD = 128
VD = 128
BLOCK = 64


EPS = 1e-06
HIGH = lax.Precision.HIGHEST


def entering(x, axis, join, neutral, backward):
    count = lax.axis_size(axis)
    place = lax.axis_index(axis)
    ahead = count - 1 - place if backward else place
    gathered = jax.tree.map(
        lambda a, kind: lax.all_gather(a.astype(kind), axis), x, (jnp.bfloat16, jnp.bfloat16)
    )
    state = jax.tree.map(lambda a, e: jnp.zeros_like(a) + jnp.asarray(e, a.dtype), x, neutral)

    def one(lap, state):
        source = count - 1 - lap if backward else lap
        return join(
            state,
            jax.tree.map(
                lambda a, own: lax.dynamic_index_in_dim(a, source, 0, False).astype(own.dtype),
                gathered,
                x,
            ),
        )

    return lax.fori_loop(0, ahead, one, state)


def padded_2(cells, sides, width):
    for axis, dim in sides:
        count = lax.axis_size(axis)
        ends = count - 1
        head = lax.slice_in_dim(cells, 0, width, axis=dim)
        tail = lax.slice_in_dim(cells, cells.shape[dim] - width, cells.shape[dim], axis=dim)
        cells = jnp.concatenate(
            [
                lax.ppermute(tail, axis, [(i, (i + 1) % count) for i in range(ends)]),
                cells,
                lax.ppermute(head, axis, [((i + 1) % count, i) for i in range(ends)]),
            ],
            axis=dim,
        )
    return cells


def block_pass(queries, key_rows, value_rows, log_gate):
    heads_n, length_n, key_dim = queries.shape
    value_dim = value_rows.shape[-1]
    blocks = length_n // BLOCK

    def split_blocks(tensor):
        return tensor.reshape(heads_n, blocks, BLOCK, tensor.shape[-1]).transpose(1, 0, 2, 3)

    def join_blocks(tensor):
        return tensor.transpose(1, 0, 2, 3).reshape(heads_n, length_n, tensor.shape[-1])

    lower_mask = jnp.tril(jnp.ones((BLOCK, BLOCK), bool))

    def advance(carried, inputs):
        states, offset = carried
        query_b, key_b, value_b, gate_b = inputs
        cumulative = jnp.cumsum(gate_b, axis=1)
        query_g = query_b * jnp.exp(cumulative)
        key_g = key_b * jnp.exp(-cumulative)
        scores = jnp.einsum("htd,hsd->hts", query_g, key_g, precision=HIGH)
        scores = jnp.where(lower_mask, scores, 0.0)
        result = jnp.einsum("hts,hse->hte", scores, value_b, precision=HIGH)
        result = result + jnp.einsum("htd,hde->hte", query_g, states, precision=HIGH)
        last_g = cumulative[:, -1, :]
        weighted = key_b * jnp.exp(last_g[:, None, :] - cumulative)
        states = jnp.exp(last_g)[:, :, None] * states + jnp.einsum(
            "hsd,hse->hde", weighted, value_b, precision=HIGH
        )
        decayed = query_b * jnp.exp(offset[:, None, :] + cumulative)
        return ((states, offset + last_g), (result, decayed))

    start_state = jnp.zeros((heads_n, key_dim, value_dim), jnp.float32)
    start_offset = jnp.zeros((heads_n, key_dim), jnp.float32)
    inputs = (
        split_blocks(queries),
        split_blocks(key_rows),
        split_blocks(value_rows),
        split_blocks(log_gate),
    )
    final_pair, outputs = lax.scan(advance, (start_state, start_offset), inputs)
    return (join_blocks(outputs[0]), join_blocks(outputs[1]), final_pair[1], final_pair[0])


def chain_combine(first_part, second_part):
    return (
        first_part[0] * second_part[0],
        second_part[0][:, :, None] * first_part[1] + second_part[1],
    )


def recurrence(query_pre, input_pre, forward_pre, backward_pre, forget_gap, log_decay, rec_gain):
    heads_local = log_decay.shape[2]
    row_count = query_pre.shape[0]

    def to_heads(tensor):
        return tensor.astype(jnp.float32).reshape(row_count, heads_local, -1).transpose(1, 0, 2)

    def gate_terms(pre_act, gap_row, decay_row):
        closing = jax.nn.sigmoid(-to_heads(pre_act)) * gap_row.reshape(heads_local, 1, -1)
        return (closing, jnp.log1p(-closing) + decay_row[:, :, None])

    queries = jax.nn.silu(to_heads(query_pre)) * KD ** (-0.5)
    values = to_heads(input_pre)
    keys_fwd, gate_fwd = gate_terms(forward_pre, forget_gap[0], log_decay[0, 0])
    keys_bwd, gate_bwd = gate_terms(backward_pre, forget_gap[1], log_decay[0, 1])
    identity = (
        jnp.ones((heads_local, KD), jnp.float32),
        jnp.zeros((heads_local, KD, VD), jnp.float32),
    )
    local_fwd, decayed_fwd, offset_fwd, state_fwd = block_pass(queries, keys_fwd, values, gate_fwd)
    incoming_fwd = entering((jnp.exp(offset_fwd), state_fwd), "sp", chain_combine, identity, False)
    forward = local_fwd + jnp.einsum("htd,hde->hte", decayed_fwd, incoming_fwd[1], precision=HIGH)
    local_bwd, decayed_bwd, offset_bwd, state_bwd = block_pass(
        jnp.flip(queries, 1), jnp.flip(keys_bwd, 1), jnp.flip(values, 1), jnp.flip(gate_bwd, 1)
    )
    incoming_bwd = entering((jnp.exp(offset_bwd), state_bwd), "sp", chain_combine, identity, True)
    backward = jnp.flip(
        local_bwd + jnp.einsum("htd,hde->hte", decayed_bwd, incoming_bwd[1], precision=HIGH), 1
    )
    joined = forward + backward
    joined = joined * lax.rsqrt(jnp.mean(joined * joined, axis=-1, keepdims=True) + EPS)
    joined = joined * rec_gain.reshape(heads_local, 1, VD)
    return joined.transpose(1, 0, 2).reshape(row_count, heads_local * VD).astype(jnp.bfloat16)


def convolve(conv_pre, glu_pre, conv_kernel, conv_gain):
    gated = (conv_pre.astype(jnp.float32) * jax.nn.sigmoid(glu_pre.astype(jnp.float32))).astype(
        jnp.bfloat16
    )
    half_width = conv_kernel.shape[0] // 2
    padded = padded_2(gated, (("sp", 0),), half_width)
    convolved = lax.conv_general_dilated(
        padded.astype(jnp.float32)[None],
        conv_kernel.astype(jnp.float32)[:, None, :],
        (1,),
        "VALID",
        dimension_numbers=("NWC", "WIO", "NWC"),
        feature_group_count=gated.shape[1],
        precision=HIGH,
    )[0]
    totals = lax.psum((jnp.sum(convolved, axis=-1), jnp.sum(convolved * convolved, axis=-1)), "tp")
    full_width = convolved.shape[1] * lax.axis_size("tp")
    mean_c = (totals[0] / full_width)[:, None]
    variance = (totals[1] / full_width)[:, None] - mean_c * mean_c
    return jax.nn.silu((convolved - mean_c) * lax.rsqrt(variance + EPS) * conv_gain).astype(
        jnp.bfloat16
    )


def body(
    tokens,
    norm_gain,
    rec_query,
    rec_input,
    rec_forward,
    rec_backward,
    forget_gap,
    log_decay,
    rec_gain,
    conv_value,
    conv_gate,
    conv_kernel,
    conv_gain,
    out_rec,
    out_conv,
):
    row_values = tokens[0].astype(jnp.float32)
    normed = row_values * lax.rsqrt(jnp.mean(row_values * row_values, axis=-1, keepdims=True) + EPS)
    normed = (normed * norm_gain).astype(jnp.bfloat16)
    whole = lax.all_gather(normed, "tp", axis=0, tiled=True)
    row_count = whole.shape[0]
    pieces = (
        lax.all_gather(rec_query, "sp", axis=0, tiled=True),
        lax.all_gather(rec_input, "sp", axis=0, tiled=True),
        lax.all_gather(rec_forward, "sp", axis=0, tiled=True),
        lax.all_gather(rec_backward, "sp", axis=0, tiled=True),
        lax.all_gather(conv_value, "sp", axis=0, tiled=True),
        lax.all_gather(conv_gate, "sp", axis=0, tiled=True),
    )
    results = tuple(
        (
            jnp.dot(whole, weight_piece, preferred_element_type=jnp.float32)
            for weight_piece in pieces
        )
    )
    projected = tuple((result.astype(jnp.bfloat16) for result in results))
    rec_out = recurrence(
        projected[0], projected[1], projected[2], projected[3], forget_gap, log_decay, rec_gain
    )
    conv_out = convolve(projected[4], projected[5], conv_kernel, conv_gain)
    both_out = jnp.concatenate([rec_out, conv_out], axis=1)
    out_local = jnp.concatenate([out_rec, out_conv], axis=0)
    full_columns = lax.all_gather(out_local, "sp", axis=1, tiled=True)
    own_rows = row_count // lax.axis_size("tp")
    rows_part = lax.slice_in_dim(both_out, 0, own_rows * lax.axis_size("tp"), axis=0)
    mixed = lax.psum_scatter(
        jnp.dot(rows_part, full_columns, preferred_element_type=jnp.float32).astype(jnp.bfloat16),
        "tp",
        scatter_dimension=0,
        tiled=True,
    )
    return mixed[None]


MESH = pl.DeviceIdType.MESH
PACK = 8


def dot_as(a, b, ca, cb, precision=HIGH):
    return lax.dot_general(
        a, b, (((ca,), (cb,)), ((), ())), precision=precision, preferred_element_type=jnp.float32
    )


PIECES = (2, 4)
TSUB = 2
LAG = 4
OUTS = 4
(
    PARAMS, DECAY, _, TOKENS, TOKENS_ON, WEIGHTS, OWN, ACROSS, BESIDE, OUT_OWN, OUT, OUT_ACROSS,
    OUT_BESIDE, GIVE, HALO, STATE, STATS, MIXED, GROUPS,
) = range(19)


def pair_kernel(
    tokens_in, gain_in, w0, w1, w2, w3, w4, w5, decay_in, gap_in, rgain_in, cgain_in, taps_in,
    out_r, out_c, o_ref, decay_v, gap_v, rgain_v, cgain_v, taps_v, tokens, gain,
    xs, x, wbuf, ow, pack, pk, lds, ld, dec, proj, gp, halo_s, halo_r, st_s, st_in, cacc, stat,
    yout, ya, mo, fin, ini, snd, w_own, w_recv, y_recv, d_recv, t_recv, p_recv, l_recv, h_recv,
    s_recv, c_recv, a_recv, o_own, o_recv, q_recv, g_recv, f_recv,
):
    s = lax.axis_index("sp")
    f = lax.axis_index("fs")
    t = lax.axis_index("tp")
    other = 1 - t
    col = lax.rem(f, 2)
    row = f // 2
    part = s // 2
    pair = lax.rem(s, 2)
    near = s + 1 - 2 * pair
    far = lax.rem(s + 2, 4)
    cross = 3 - s
    fx = f + 1 - 2 * col
    fy = lax.rem(f + 2, 4)
    fd = 3 - f
    head = 2 * pair + col
    rows = tokens.shape[1]
    span = 2 * rows
    total = 2 * span
    width = KD
    weights = (w0, w1, w2, w3, w4, w5)
    kslice = w0.shape[0]
    fourth = kslice // 4
    kinds = (range(4, 6), range(0, 4))
    half = out_r.shape[0]
    quarter = half // 4
    cols = out_r.shape[1]
    groups = 4 * width
    ways = (near, 2 - part, 3 - 3 * part)
    NEAR, INNER, OUTER = range(3)
    mine = OUTER - (pair - part) * (pair - part)
    own_col = t == col
    own_weights = t == pair

    def at(sp=s, fs=f, tp=t):
        return {"sp": sp, "fs": fs, "tp": tp}

    def remote(src, dst, send, recv, to):
        return pltpu.make_async_remote_copy(
            src_ref=src, dst_ref=dst, send_sem=send, recv_sem=recv, device_id=to,
            device_id_type=MESH,
        )

    def when(cond, act):
        if cond is None:
            act()
        else:
            pl.when(cond)(act)

    def send(src, dst, group, recv, to, cond=None):
        when(cond, remote(src, dst, snd.at[group], recv, to).start)

    def arrived(ref, sem, cond=None):
        when(cond, pltpu.make_async_copy(ref, ref, sem).wait)

    def aligned(start, size, unit):
        return pl.ds(pl.multiple_of(start, unit), size)

    entry = [
        pltpu.make_async_copy(src, dst, ini.at[i])
        for i, (src, dst) in enumerate(
            (
                (tokens_in, tokens), (gain_in, gain), (decay_in, decay_v), (gap_in, gap_v),
                (rgain_in, rgain_v), (cgain_in, cgain_v), (taps_in, taps_v),
            )
        )
    ]
    for copy in entry:
        copy.start()

    def slot(place, core, k=None):
        if k is None:
            return aligned(place * span + core * rows, rows, rows)
        step = rows // TSUB
        return aligned(place * span + core * rows + k * step, step, step)

    barrier = pltpu.get_barrier_semaphore()
    greet = [at(sp=lax.rem(s + d, 4), tp=lax.rem(t + c, 2)) for d in range(4) for c in range(2) if d or c]
    greet += [at(sp=z, fs=fx, tp=lax.rem(t + c, 2)) for z in (s, near) for c in range(2)]
    greet += [at(fs=fy), at(fs=fd)]
    for to in greet:
        pl.semaphore_signal(barrier, inc=1, device_id=to, device_id_type=MESH)

    for copy in entry:
        copy.wait()
    values = tokens[0].astype(jnp.float32)
    normed = values * lax.rsqrt(jnp.mean(values * values, axis=-1, keepdims=True) + EPS)
    normed = (normed * gain[...]).astype(jnp.bfloat16)
    xs[...] = normed

    @pl.when(own_col)
    def _():
        x[slot(pair, t), :] = normed

    taps_n = taps_v.shape[0]
    at_col = aligned(col * width, width, width)
    pack[0:2, :] = gap_v[:, at_col]
    pack[2:3, :] = rgain_v[:, at_col]
    pack[3:4, :] = cgain_v[:, at_col]
    pack[4:PACK, :] = jnp.zeros((PACK - 4, width), jnp.float32)
    pack[PACK : PACK + taps_n, :] = taps_v[:, at_col].astype(jnp.float32)
    for j in range(2):
        lds[j, 0:2, :] = decay_v[0, :, j, :]
        lds[j, 2:PACK, :] = jnp.zeros((PACK - 2, span), jnp.float32)
    pl.semaphore_wait(barrier, len(greet))

    def piece(kind, place, side, core, i):
        size = fourth // PIECES[kind]
        at_cols = pl.ds(kinds[kind].start * width, len(kinds[kind]) * width)
        return wbuf.at[
            aligned(place * kslice + (side * 2 + core) * fourth + i * size, size, size), at_cols
        ]

    def flag(kind, way, i):
        return (PIECES[0] * 3 if kind else 0) + way * PIECES[kind] + i

    def send_weights(kind, i):
        size = fourth // PIECES[kind]
        for place, way in ((far, mine), (cross, mine), (near, NEAR)):
            for core in range(2):
                src_rows = aligned((row * 2 + core) * fourth + i * size, size, size)
                dst_rows = aligned(s * kslice + (row * 2 + core) * fourth + i * size, size, size)
                for m in kinds[kind]:
                    send(
                        weights[m].at[src_rows, at_col],
                        wbuf.at[dst_rows, pl.ds(m * width, width)],
                        WEIGHTS, w_recv.at[flag(kind, way, i)], at(sp=place, tp=core),
                        own_weights if place is far else jnp.logical_not(own_weights),
                    )

    @pl.when(own_weights)
    def _():
        pk[...] = pack[...]

    send(pack, pk, PARAMS, p_recv, at(tp=other), own_weights)
    for j in range(2):
        to = at(sp=2 * part + t, fs=2 * row + j, tp=col)
        here = own_weights & (col == j) & own_col

        @pl.when(here)
        def _(j=j):
            pltpu.make_async_copy(lds.at[j], ld.at[pair], l_recv.at[pair]).start()

        send(lds.at[j], ld.at[pair], DECAY + j, l_recv.at[pair], to, jnp.logical_not(here))

    def send_tokens(k):
        step = rows // TSUB
        src = xs.at[pl.ds(k * step, step)]
        dst = x.at[slot(pair, t, k)]
        sem = t_recv.at[pair, t, k]
        send(src, dst, TOKENS, sem, at(sp=near, tp=col))
        send(src, dst, TOKENS, sem, at(fs=fx, tp=col))
        send(src, dst, TOKENS_ON, sem, at(tp=col), jnp.logical_not(own_col))

    own_rows = aligned(s * kslice, kslice, kslice)
    for m in range(6):

        @pl.when(own_weights)
        def _(m=m):
            src = weights[m].at[:, at_col]
            dst = wbuf.at[own_rows, pl.ds(m * width, width)]
            kind = 0 if m in kinds[0] else 1
            remote(src, dst, snd.at[OWN], w_own.at[kind], at(tp=other)).start()
            pltpu.make_async_copy(src, dst, w_own.at[kind]).start()

    def out_cols(place):
        return aligned(place * cols, cols, cols)

    for which, ref in enumerate((out_r, out_c)):
        dst = ow.at[which, aligned(t * half, half, half), pl.ds(0, cols)]
        pltpu.make_async_copy(ref, dst, o_own.at[0]).start()
        send(ref, dst, OUT_OWN, o_own.at[1], at(tp=other))

    def relay_tokens(k):
        scope(f"T{k}")
        for core in range(2):
            ref = x.at[slot(1 - pair, core, k)]
            arrived(ref, t_recv.at[1 - pair, core, k], own_col)
            send(ref, ref, TOKENS_ON, t_recv.at[1 - pair, core, k], at(fs=fx), own_col)

    def first_hop(kind, way, i):
        scope(f"A{kind}{way}{i}")
        ref = piece(kind, ways[way], row, t, i)
        arrived(ref, w_recv.at[flag(kind, way, i)])
        send(ref, ref, ACROSS, y_recv.at[flag(kind, way, i)], at(fs=fy))
        send(ref, ref, BESIDE, d_recv.at[kind], at(tp=other))

    def second_hop(kind, way, i):
        scope(f"B{kind}{way}{i}")
        ref = piece(kind, ways[way], 1 - row, t, i)
        arrived(ref, y_recv.at[flag(kind, way, i)])
        send(ref, ref, BESIDE, d_recv.at[kind], at(tp=other))

    def weights_wait(kind):
        at_cols = pl.ds(kinds[kind].start * width, len(kinds[kind]) * width)
        arrived(wbuf.at[own_rows, at_cols], w_own.at[kind])
        arrived(wbuf.at[pl.ds(0, 6 * fourth), at_cols], d_recv.at[kind])

    cut = quarter // (OUTS // 2)

    def out_part(core, quart, k):
        return ow.at[
            k // (OUTS // 2),
            aligned(core * half + quart * quarter + k % (OUTS // 2) * cut, cut, cut),
            pl.ds(cols, cols),
        ]

    def send_out(k):
        src = (out_r, out_c)[k // (OUTS // 2)].at[
            aligned(f * quarter + k % (OUTS // 2) * cut, cut, cut), :
        ]
        send(src, out_part(t, f, k), OUT, o_recv.at[k], at(sp=far))

    def out_first(k):
        scope(f"X{k}")
        ref = out_part(t, f, k)
        arrived(ref, o_recv.at[k])
        send(ref, ref, OUT_ACROSS, q_recv.at[k, 0], at(fs=fx))
        send(ref, ref, OUT_ACROSS, q_recv.at[k, 1], at(fs=fy))
        send(ref, ref, OUT_BESIDE, g_recv, at(tp=other))

    def out_second(k):
        scope(f"Y{k}")
        for j, (source, to) in enumerate(((fx, fy), (fy, fx))):
            ref = out_part(t, source, k)
            arrived(ref, q_recv.at[k, j])
            if k % 2 == j:
                send(ref, ref, OUT_ACROSS, q_recv.at[k, 2], at(fs=to))
            send(ref, ref, OUT_BESIDE, g_recv, at(tp=other))

    def out_third(k):
        scope(f"Z{k}")
        ref = out_part(t, fd, k)
        arrived(ref, q_recv.at[k, 2])
        send(ref, ref, OUT_BESIDE, g_recv, at(tp=other))

    def run(step, *pieces):
        for k in pieces:
            step(k)

    def project(n0):
        at_n = pl.ds(n0 * 2 * width, 2 * width)
        proj[:, at_n] = jnp.dot(
            x[...], wbuf[:, at_n], preferred_element_type=jnp.float32
        ).astype(jnp.bfloat16)

    for k in range(TSUB):
        send_tokens(k)
    for kind in range(2):
        for i in range(PIECES[kind]):
            send_weights(kind, i)
    bf = jnp.bfloat16
    blocks = total // BLOCK
    pad = 16

    def decay_columns():
        scope("dec")
        for place in range(2):
            arrived(ld.at[place], l_recv.at[place])
        arrived(pk, p_recv, jnp.logical_not(own_weights))
        pick = lax.broadcasted_iota(jnp.int32, (PACK, width), 0)
        for place in range(2):
            for d in range(2):
                dec[d, pl.ds(place * span, span), :] = dot_as(
                    ld[place], (pick == d).astype(jnp.float32), 0, 0
                )

    def conv_open():
        scope("tokwait")
        for k in range(TSUB):
            for place in (pair, 1 - pair):
                for core in range(2):
                    local = own_col & (place == pair) & (t == core)
                    done = own_col & (place == 1 - pair)
                    skip = local | done if place is not pair else local
                    arrived(x.at[slot(place, core, k)], t_recv.at[place, core, k], jnp.logical_not(skip))
        scope("cwait")
        weights_wait(0)
        scope("projectc")
        project(2)
        scope("gate")
        conv_pre = proj[:, 4 * width : 5 * width].astype(jnp.float32)
        glu_pre = proj[:, 5 * width : 6 * width].astype(jnp.float32)
        gated = (conv_pre * jax.nn.sigmoid(glu_pre)).astype(jnp.bfloat16)
        gp[pad : pad + total, :] = gated.astype(jnp.float32)
        halo_s[...] = jnp.where(part == 0, gated[total - pad :], gated[0:pad])
        send(halo_s, halo_r, HALO, h_recv, at(sp=far))
        for k in range(OUTS):
            send_out(k)

    def conv_close():
        scope("conv")
        arrived(halo_r, h_recv)
        halo = halo_r[...].astype(jnp.float32)
        none = jnp.zeros((pad, width), jnp.float32)
        gp[0:pad, :] = jnp.where(part == 1, halo, none)
        gp[pad + total : 2 * pad + total, :] = jnp.where(part == 0, halo, none)
        first = pad - taps_n // 2
        for b in range(blocks):
            acc = jnp.zeros((BLOCK, width), jnp.float32)
            for j in range(taps_n):
                acc = acc + pk[PACK + j : PACK + j + 1, :] * gp[pl.ds(b * BLOCK + first + j, BLOCK), :]
            cacc[pl.ds(b * BLOCK, BLOCK), :] = acc
        conv = cacc[...]
        ones = jnp.ones((8, width), jnp.float32)
        stat[head, 0] = dot_as(ones, conv, 1, 1)
        stat[head, 1] = dot_as(ones, conv * conv, 1, 1)
        own_stat = stat.at[head]
        send(own_stat, own_stat, STATS, c_recv, at(fs=fx))
        send(own_stat, own_stat, STATS, c_recv, at(sp=near))
        send(own_stat, own_stat, STATS, c_recv, at(sp=near, fs=fx))

    order = [
        (0, INNER, 0), (0, INNER, 1), (1, INNER, 0), (0, OUTER, 0), (0, NEAR, 0), (0, OUTER, 1),
        (0, NEAR, 1), (1, INNER, 1), (1, OUTER, 0), (1, NEAR, 0), (1, INNER, 2), (1, OUTER, 1),
        (1, NEAR, 1), (1, INNER, 3), (1, OUTER, 2), (1, NEAR, 2), (1, OUTER, 3), (1, NEAR, 3),
    ]
    for k, hop in enumerate(order):
        if k == 2:
            relay_tokens(0)
        if k == 3:
            relay_tokens(1)
        first_hop(*hop)
        if k >= LAG:
            second_hop(*order[k - LAG])
        if k == 5:
            decay_columns()
        if k == 7 + LAG:
            conv_open()
    run(out_first, 0, 1)
    conv_close()
    for hop in order[-LAG:]:
        second_hop(*hop)
    run(out_first, 2, 3)
    scope("rwait")
    weights_wait(1)
    scope("projectr")
    project(1)
    project(0)
    scope("states")
    def f32(n0):
        return proj[:, n0 * width : (n0 + 1) * width].astype(jnp.float32)

    query_pre = f32(0)
    query = query_pre * jax.nn.sigmoid(query_pre) * width ** (-0.5)
    value = proj[:, width : 2 * width]
    keys, gates = [], []
    for d in range(2):
        key = pk[d : d + 1, :] * jax.nn.sigmoid(-f32(2 + d))
        keys.append(key)
        gates.append(jnp.log1p(-key) + dec[d])
    row_i = lax.broadcasted_iota(jnp.int32, (total, total), 0)
    col_i = lax.broadcasted_iota(jnp.int32, (total, total), 1)
    same = (row_i // BLOCK) == (col_i // BLOCK)
    lower = same & (row_i >= col_i)
    upper = same & (row_i <= col_i)
    both = jnp.concatenate(gates, axis=1)
    high = both.astype(bf)
    low = (both - high.astype(jnp.float32)).astype(bf)
    tri = lower.astype(jnp.float32).astype(bf)
    sums = jnp.dot(tri, high, preferred_element_type=jnp.float32) + jnp.dot(
        tri, low, preferred_element_type=jnp.float32
    )
    lasts = [sums[b * BLOCK + BLOCK - 1 : (b + 1) * BLOCK, :] for b in range(blocks)]

    def spread_rows(parts):
        return jnp.concatenate([jnp.broadcast_to(a, (BLOCK, width)) for a in parts], axis=0)

    last = [[a[:, d * width : (d + 1) * width] for a in lasts] for d in range(2)]
    last_rows = [spread_rows(last[d]) for d in range(2)]
    cum_f = sums[:, 0:width]
    cum_b = last_rows[1] - sums[:, width:] + gates[1]
    cums = (cum_f, cum_b)
    query_g = [(query * jnp.exp(cums[d])).astype(bf) for d in range(2)]
    key_g = [(keys[d] * jnp.exp(-cums[d])).astype(bf) for d in range(2)]
    weighted = jnp.concatenate(
        [(keys[d] * jnp.exp(last_rows[d] - cums[d])).astype(bf) for d in range(2)], axis=1
    )
    outer = [
        lax.dot_general(
            value[b * BLOCK : (b + 1) * BLOCK], weighted[b * BLOCK : (b + 1) * BLOCK],
            (((0,), (0,)), ((), ())), preferred_element_type=jnp.float32,
        )
        for b in range(blocks)
    ]
    states = [[None] * blocks, [None] * blocks]
    ends, offsets = [], [[None] * blocks, [None] * blocks]
    for d in range(2):
        state = jnp.zeros((width, width), jnp.float32)
        offset = jnp.zeros((1, width), jnp.float32)
        for b in range(blocks) if d == 0 else range(blocks - 1, -1, -1):
            states[d][b] = state
            offsets[d][b] = offset
            state = state * jnp.exp(last[d][b]) + outer[b][:, d * width : (d + 1) * width]
            offset = offset + last[d][b]
        ends.append(state)
    st_s[...] = jnp.where(part == 0, ends[0], ends[1]).astype(bf)
    send(st_s, st_in, STATE, s_recv, at(sp=far))


    run(out_second, 0, 1)
    scope("scores")
    scores = [
        lax.dot_general(
            query_g[d], key_g[d], (((1,), (1,)), ((), ())), preferred_element_type=jnp.float32
        )
        for d in range(2)
    ]
    scores = (jnp.where(lower, scores[0], 0.0) + jnp.where(upper, scores[1], 0.0)).astype(bf)
    inner = jnp.dot(scores, value, preferred_element_type=jnp.float32)
    carried = jnp.concatenate(
        [
            lax.dot_general(
                jnp.concatenate([q[b * BLOCK : (b + 1) * BLOCK] for q in query_g], axis=1),
                jnp.concatenate([states[d][b].astype(bf) for d in range(2)], axis=1),
                (((1,), (1,)), ((), ())), preferred_element_type=jnp.float32,
            )
            for b in range(blocks)
        ],
        axis=0,
    )
    reach = jnp.where(
        part == 1, spread_rows(offsets[0]) + cum_f, spread_rows(offsets[1]) + cum_b
    )
    query_in = (query * jnp.exp(reach)).astype(bf)
    def mix(which, out):
        for core in range(2):
            for place in range(2):
                at_row = place * span + core * rows
                yout[which, pl.ds(core * span + place * rows, rows), :] = out[
                    at_row : at_row + rows
                ].astype(bf)
        dst = ya.at[:, aligned(which * groups + head * width, width, width)]
        for place in range(2):
            for core in range(2):
                src = yout.at[which, pl.ds(core * span, span)]
                here = own_col & (pair == place) & (t == core)

                @pl.when(here)
                def _(src=src):
                    pltpu.make_async_copy(src, dst, a_recv.at[which]).start()

                send(
                    src, dst, MIXED, a_recv.at[which],
                    at(sp=2 * part + place, fs=2 * row + t, tp=core), jnp.logical_not(here),
                )

    scope("statx")
    arrived(stat.at[pl.ds(0, 3)], c_recv)
    scope("cnorm")
    stats = (stat[0] + stat[1] + stat[2] + stat[3]) / groups
    mean_r = stats[0]
    inv_r = lax.rsqrt(stats[1] - mean_r * mean_r + EPS)
    eighth = jnp.full((8, width), 0.125, jnp.float32)
    mean_c = dot_as(mean_r, eighth, 0, 0)
    inv_c = dot_as(inv_r, eighth, 0, 0)
    out = (cacc[...] - mean_c) * inv_c * pk[3:4, :]
    mix(1, out * jax.nn.sigmoid(out))

    run(out_second, 2, 3)
    scope("statein")
    arrived(st_in, s_recv)
    scope("recnorm")
    joined = inner + carried + lax.dot_general(
        query_in, st_in[...], (((1,), (1,)), ((), ())), preferred_element_type=jnp.float32
    )
    joined = joined * lax.rsqrt(jnp.mean(joined * joined, axis=-1, keepdims=True) + EPS)
    mix(0, joined * pk[2:3, :])

    run(out_third, 0, 1, 2, 3)
    scope("ywait1")
    arrived(ya.at[:, pl.ds(0, groups)], a_recv.at[1])
    for k in range(2):
        arrived(ow.at[:, pl.ds(0, half), pl.ds(0, cols)], o_own.at[k])
    scope("ywait0")
    arrived(ya.at[:, pl.ds(0, groups)], a_recv.at[0])
    near_rows = aligned((1 - pair) * rows, rows, rows)
    for k in range(2):
        scope(f"outmm{k}")
        if k == 1:
            arrived(ow.at[:, pl.ds(0, half), pl.ds(0, cols)], g_recv)
        at_n = pl.ds(k * cols, cols)
        acc = jnp.dot(ya[:, 0:groups], ow[0, :, at_n], preferred_element_type=jnp.float32)
        acc = acc + jnp.dot(ya[:, groups:], ow[1, :, at_n], preferred_element_type=jnp.float32)
        mo[:, at_n] = acc.astype(bf)
        send(mo.at[near_rows, at_n], fin.at[:, at_n], GIVE, f_recv.at[k], at(sp=near))
    own_rows = aligned(pair * rows, rows, rows)
    for k, place in enumerate((s, far)):
        o_ref[0, :, out_cols(place)] = mo[own_rows, pl.ds(k * cols, cols)]
    for k, place in enumerate((near, cross)):
        scope(f"give{k}")
        at_n = pl.ds(k * cols, cols)
        arrived(fin.at[:, at_n], f_recv.at[k])
        o_ref[0, :, out_cols(place)] = fin[:, at_n]

    scope("sendwaits")
    other_weights = jnp.logical_not(own_weights)
    other_col = jnp.logical_not(own_col)
    arrived(pack, snd.at[PARAMS], own_weights)
    for j in range(2):
        here = own_weights & (col == j) & own_col
        arrived(lds.at[j], snd.at[DECAY + j], jnp.logical_not(here))
    arrived(x.at[pl.ds(0, 2 * rows)], snd.at[TOKENS])
    arrived(x.at[pl.ds(0, 2 * rows)], snd.at[TOKENS_ON], own_col)
    arrived(x.at[pl.ds(0, rows)], snd.at[TOKENS_ON], other_col)
    arrived(wbuf.at[pl.ds(0, 2 * fourth)], snd.at[WEIGHTS], own_weights)
    arrived(wbuf.at[pl.ds(0, 4 * fourth)], snd.at[WEIGHTS], other_weights)
    arrived(wbuf.at[pl.ds(0, kslice)], snd.at[OWN], own_weights)
    arrived(wbuf.at[pl.ds(0, 3 * fourth)], snd.at[ACROSS])
    arrived(wbuf.at[pl.ds(0, 6 * fourth)], snd.at[BESIDE])
    arrived(ow.at[:, pl.ds(0, half), pl.ds(0, cols)], snd.at[OUT_OWN])
    arrived(ow.at[:, pl.ds(0, quarter), pl.ds(0, cols)], snd.at[OUT])
    arrived(ow.at[:, pl.ds(0, 3 * quarter), pl.ds(0, cols)], snd.at[OUT_ACROSS])
    arrived(ow.at[:, pl.ds(0, 4 * quarter), pl.ds(0, cols)], snd.at[OUT_BESIDE])
    arrived(halo_s, snd.at[HALO])
    arrived(st_s, snd.at[STATE])
    arrived(stat.at[pl.ds(0, 3)], snd.at[STATS])
    arrived(x.at[pl.ds(0, 6 * span * width // x.shape[1])], snd.at[MIXED], own_col)
    arrived(x.at[pl.ds(0, 8 * span * width // x.shape[1])], snd.at[MIXED], other_col)
    arrived(fin, snd.at[GIVE])
    scope(None)


def scope(name):
    pass


def pair_body(
    tokens, norm_gain, rec_query, rec_input, rec_forward, rec_backward, forget_gap,
    log_decay, rec_gain, conv_value, conv_gate, conv_kernel, conv_gain, out_rec, out_conv,
):
    rows, d = tokens.shape[1:]
    total = 4 * rows
    taps = conv_kernel.shape[0]
    width = KD
    half, cols = out_rec.shape

    bf, f32 = jnp.bfloat16, jnp.float32
    dma = pltpu.SemaphoreType.DMA
    small = (log_decay, forget_gap, rec_gain[None], conv_gain[None], conv_kernel)
    scratch = [
        *(pltpu.VMEM(a.shape, a.dtype) for a in small),
        pltpu.VMEM(tokens.shape, bf),
        pltpu.VMEM((1, d), f32),
        pltpu.VMEM((rows, d), bf),
        pltpu.VMEM((total, d), bf),
        pltpu.VMEM((d, 6 * width), bf),
        pltpu.VMEM((2, 2 * half, 2 * cols), bf),
        pltpu.VMEM((PACK + taps, width), f32),
        pltpu.VMEM((PACK + taps, width), f32),
        pltpu.VMEM((2, PACK, 2 * rows), f32),
        pltpu.VMEM((2, PACK, 2 * rows), f32),
        pltpu.VMEM((2, total, width), f32),
        pltpu.VMEM((total, 6 * width), bf),
        pltpu.VMEM((total + 32, width), f32),
        pltpu.VMEM((16, width), bf),
        pltpu.VMEM((16, width), bf),
        pltpu.VMEM((width, width), bf),
        pltpu.VMEM((width, width), bf),
        pltpu.VMEM((total, width), f32),
        pltpu.VMEM((4, 2, 8, total), f32),
        pltpu.VMEM((2, total, width), bf),
        pltpu.VMEM((2 * rows, 8 * width), bf),
        pltpu.VMEM((2 * rows, 2 * cols), bf),
        pltpu.VMEM((rows, 2 * cols), bf),
        dma((7,)), dma((GROUPS,)), dma((2,)), dma((3 * sum(PIECES),)), dma((3 * sum(PIECES),)),
        dma((2,)), dma((2, 2, TSUB)), dma(()), dma((2,)), dma(()),
        dma(()), dma(()), dma((2,)), dma((2,)), dma((OUTS,)), dma((OUTS, 3)), dma(()), dma((2,)),
    ]
    return pl.pallas_call(
        pair_kernel,
        out_shape=jax.ShapeDtypeStruct((1, rows, d), bf),
        in_specs=[pl.BlockSpec(memory_space=pl.ANY)] * 15,
        out_specs=pl.BlockSpec(memory_space=pltpu.VMEM),
        scratch_shapes=scratch,
        compiler_params=pltpu.CompilerParams(
            collective_id=0, has_side_effects=True, vmem_limit_bytes=60 * 1024 * 1024
        ),
    )(
        tokens, norm_gain[None], rec_query, rec_input, rec_forward, rec_backward, conv_value,
        conv_gate, *small, out_rec, out_conv,
    )


def fits(n, nf, nt, tokens, rec_query, log_decay, conv_value, conv_kernel, out_rec):
    heads = log_decay.shape[2]
    rows = tokens.shape[1] // (n * nt)
    return (
        nt == 2
        and n == 4
        and nf == 4
        and n == heads
        and tokens.shape[0] == nf
        and rec_query.shape[1] == heads * KD
        and conv_value.shape[1] == heads * VD
        and KD == VD
        and 2 * rows == KD
        and rows % (16 * TSUB) == 0
        and rec_query.shape[0] % (n * 4 * max(PIECES) * 16) == 0
        and out_rec.shape[0] % (nt * nf * 16) == 0
        and conv_kernel.shape[0] // 2 <= 15
    )


def layer(mesh, *args):
    n, nf, nt = (mesh.shape[a] for a in ("sp", "fs", "tp"))
    fast = fits(n, nf, nt, args[0], args[2], args[7], args[9], args[11], args[13])
    return sharded(mesh, pair_body if fast else body)(*args)


def solution(mesh):
    return functools.partial(layer, mesh)


def sharded(mesh, body):
    return jax.shard_map(
        body,
        mesh=mesh,
        in_specs=(
            P("fs", ("sp", "tp"), None),
            P(),
            P("sp", "tp"),
            P("sp", "tp"),
            P("sp", "tp"),
            P("sp", "tp"),
            P(None, "tp"),
            P("fs", None, "tp", "sp"),
            P("tp"),
            P("sp", "tp"),
            P("sp", "tp"),
            P(None, "tp"),
            P("tp"),
            P("tp", "sp"),
            P("tp", "sp"),
        ),
        out_specs=P("fs", ("sp", "tp"), None),
        check_vma=False,
    )
```

```python
import functools

import jax
import jax.numpy as jnp
from jax import lax
from jax.experimental import pallas as pl
from jax.experimental.pallas import tpu as pltpu
from jax.sharding import PartitionSpec as P

KD = 128
VD = 128
BLOCK = 64


EPS = 1e-06
HIGH = lax.Precision.HIGHEST


def entering(x, axis, join, neutral, backward):
    count = lax.axis_size(axis)
    place = lax.axis_index(axis)
    ahead = count - 1 - place if backward else place
    gathered = jax.tree.map(
        lambda a, kind: lax.all_gather(a.astype(kind), axis), x, (jnp.bfloat16, jnp.bfloat16)
    )
    state = jax.tree.map(lambda a, e: jnp.zeros_like(a) + jnp.asarray(e, a.dtype), x, neutral)

    def one(lap, state):
        source = count - 1 - lap if backward else lap
        return join(
            state,
            jax.tree.map(
                lambda a, own: lax.dynamic_index_in_dim(a, source, 0, False).astype(own.dtype),
                gathered,
                x,
            ),
        )

    return lax.fori_loop(0, ahead, one, state)


def padded_2(cells, sides, width):
    for axis, dim in sides:
        count = lax.axis_size(axis)
        ends = count - 1
        head = lax.slice_in_dim(cells, 0, width, axis=dim)
        tail = lax.slice_in_dim(cells, cells.shape[dim] - width, cells.shape[dim], axis=dim)
        cells = jnp.concatenate(
            [
                lax.ppermute(tail, axis, [(i, (i + 1) % count) for i in range(ends)]),
                cells,
                lax.ppermute(head, axis, [((i + 1) % count, i) for i in range(ends)]),
            ],
            axis=dim,
        )
    return cells


def block_pass(queries, key_rows, value_rows, log_gate):
    heads_n, length_n, key_dim = queries.shape
    value_dim = value_rows.shape[-1]
    blocks = length_n // BLOCK

    def split_blocks(tensor):
        return tensor.reshape(heads_n, blocks, BLOCK, tensor.shape[-1]).transpose(1, 0, 2, 3)

    def join_blocks(tensor):
        return tensor.transpose(1, 0, 2, 3).reshape(heads_n, length_n, tensor.shape[-1])

    lower_mask = jnp.tril(jnp.ones((BLOCK, BLOCK), bool))

    def advance(carried, inputs):
        states, offset = carried
        query_b, key_b, value_b, gate_b = inputs
        cumulative = jnp.cumsum(gate_b, axis=1)
        query_g = query_b * jnp.exp(cumulative)
        key_g = key_b * jnp.exp(-cumulative)
        scores = jnp.einsum("htd,hsd->hts", query_g, key_g, precision=HIGH)
        scores = jnp.where(lower_mask, scores, 0.0)
        result = jnp.einsum("hts,hse->hte", scores, value_b, precision=HIGH)
        result = result + jnp.einsum("htd,hde->hte", query_g, states, precision=HIGH)
        last_g = cumulative[:, -1, :]
        weighted = key_b * jnp.exp(last_g[:, None, :] - cumulative)
        states = jnp.exp(last_g)[:, :, None] * states + jnp.einsum(
            "hsd,hse->hde", weighted, value_b, precision=HIGH
        )
        decayed = query_b * jnp.exp(offset[:, None, :] + cumulative)
        return ((states, offset + last_g), (result, decayed))

    start_state = jnp.zeros((heads_n, key_dim, value_dim), jnp.float32)
    start_offset = jnp.zeros((heads_n, key_dim), jnp.float32)
    inputs = (
        split_blocks(queries),
        split_blocks(key_rows),
        split_blocks(value_rows),
        split_blocks(log_gate),
    )
    final_pair, outputs = lax.scan(advance, (start_state, start_offset), inputs)
    return (join_blocks(outputs[0]), join_blocks(outputs[1]), final_pair[1], final_pair[0])


def chain_combine(first_part, second_part):
    return (
        first_part[0] * second_part[0],
        second_part[0][:, :, None] * first_part[1] + second_part[1],
    )


def recurrence(query_pre, input_pre, forward_pre, backward_pre, forget_gap, log_decay, rec_gain):
    heads_local = log_decay.shape[2]
    row_count = query_pre.shape[0]

    def to_heads(tensor):
        return tensor.astype(jnp.float32).reshape(row_count, heads_local, -1).transpose(1, 0, 2)

    def gate_terms(pre_act, gap_row, decay_row):
        closing = jax.nn.sigmoid(-to_heads(pre_act)) * gap_row.reshape(heads_local, 1, -1)
        return (closing, jnp.log1p(-closing) + decay_row[:, :, None])

    queries = jax.nn.silu(to_heads(query_pre)) * KD ** (-0.5)
    values = to_heads(input_pre)
    keys_fwd, gate_fwd = gate_terms(forward_pre, forget_gap[0], log_decay[0, 0])
    keys_bwd, gate_bwd = gate_terms(backward_pre, forget_gap[1], log_decay[0, 1])
    identity = (
        jnp.ones((heads_local, KD), jnp.float32),
        jnp.zeros((heads_local, KD, VD), jnp.float32),
    )
    local_fwd, decayed_fwd, offset_fwd, state_fwd = block_pass(queries, keys_fwd, values, gate_fwd)
    incoming_fwd = entering((jnp.exp(offset_fwd), state_fwd), "sp", chain_combine, identity, False)
    forward = local_fwd + jnp.einsum("htd,hde->hte", decayed_fwd, incoming_fwd[1], precision=HIGH)
    local_bwd, decayed_bwd, offset_bwd, state_bwd = block_pass(
        jnp.flip(queries, 1), jnp.flip(keys_bwd, 1), jnp.flip(values, 1), jnp.flip(gate_bwd, 1)
    )
    incoming_bwd = entering((jnp.exp(offset_bwd), state_bwd), "sp", chain_combine, identity, True)
    backward = jnp.flip(
        local_bwd + jnp.einsum("htd,hde->hte", decayed_bwd, incoming_bwd[1], precision=HIGH), 1
    )
    joined = forward + backward
    joined = joined * lax.rsqrt(jnp.mean(joined * joined, axis=-1, keepdims=True) + EPS)
    joined = joined * rec_gain.reshape(heads_local, 1, VD)
    return joined.transpose(1, 0, 2).reshape(row_count, heads_local * VD).astype(jnp.bfloat16)


def convolve(conv_pre, glu_pre, conv_kernel, conv_gain):
    gated = (conv_pre.astype(jnp.float32) * jax.nn.sigmoid(glu_pre.astype(jnp.float32))).astype(
        jnp.bfloat16
    )
    half_width = conv_kernel.shape[0] // 2
    padded = padded_2(gated, (("sp", 0),), half_width)
    convolved = lax.conv_general_dilated(
        padded.astype(jnp.float32)[None],
        conv_kernel.astype(jnp.float32)[:, None, :],
        (1,),
        "VALID",
        dimension_numbers=("NWC", "WIO", "NWC"),
        feature_group_count=gated.shape[1],
        precision=HIGH,
    )[0]
    totals = lax.psum((jnp.sum(convolved, axis=-1), jnp.sum(convolved * convolved, axis=-1)), "tp")
    full_width = convolved.shape[1] * lax.axis_size("tp")
    mean_c = (totals[0] / full_width)[:, None]
    variance = (totals[1] / full_width)[:, None] - mean_c * mean_c
    return jax.nn.silu((convolved - mean_c) * lax.rsqrt(variance + EPS) * conv_gain).astype(
        jnp.bfloat16
    )


def body(
    tokens,
    norm_gain,
    rec_query,
    rec_input,
    rec_forward,
    rec_backward,
    forget_gap,
    log_decay,
    rec_gain,
    conv_value,
    conv_gate,
    conv_kernel,
    conv_gain,
    out_rec,
    out_conv,
):
    row_values = tokens[0].astype(jnp.float32)
    normed = row_values * lax.rsqrt(jnp.mean(row_values * row_values, axis=-1, keepdims=True) + EPS)
    normed = (normed * norm_gain).astype(jnp.bfloat16)
    whole = lax.all_gather(normed, "tp", axis=0, tiled=True)
    row_count = whole.shape[0]
    pieces = (
        lax.all_gather(rec_query, "sp", axis=0, tiled=True),
        lax.all_gather(rec_input, "sp", axis=0, tiled=True),
        lax.all_gather(rec_forward, "sp", axis=0, tiled=True),
        lax.all_gather(rec_backward, "sp", axis=0, tiled=True),
        lax.all_gather(conv_value, "sp", axis=0, tiled=True),
        lax.all_gather(conv_gate, "sp", axis=0, tiled=True),
    )
    results = tuple(
        (
            jnp.dot(whole, weight_piece, preferred_element_type=jnp.float32)
            for weight_piece in pieces
        )
    )
    projected = tuple((result.astype(jnp.bfloat16) for result in results))
    rec_out = recurrence(
        projected[0], projected[1], projected[2], projected[3], forget_gap, log_decay, rec_gain
    )
    conv_out = convolve(projected[4], projected[5], conv_kernel, conv_gain)
    both_out = jnp.concatenate([rec_out, conv_out], axis=1)
    out_local = jnp.concatenate([out_rec, out_conv], axis=0)
    full_columns = lax.all_gather(out_local, "sp", axis=1, tiled=True)
    own_rows = row_count // lax.axis_size("tp")
    rows_part = lax.slice_in_dim(both_out, 0, own_rows * lax.axis_size("tp"), axis=0)
    mixed = lax.psum_scatter(
        jnp.dot(rows_part, full_columns, preferred_element_type=jnp.float32).astype(jnp.bfloat16),
        "tp",
        scatter_dimension=0,
        tiled=True,
    )
    return mixed[None]


MESH = pl.DeviceIdType.MESH
PACK = 8


def dot_as(a, b, ca, cb, precision=HIGH):
    return lax.dot_general(
        a, b, (((ca,), (cb,)), ((), ())), precision=precision, preferred_element_type=jnp.float32
    )


PIECES = (2, 4, 1)
TSUB = 2
LAG = 6
OUTS = 4
(
    PARAMS, DECAY, _, TOKENS, TOKENS_ON, WEIGHTS, OWN, ACROSS, BESIDE, OUT_OWN, OUT, OUT_ACROSS,
    OUT_BESIDE, GIVE, HALO, STATE, STATS, MIXED, GROUPS,
) = range(19)


def pair_kernel(
    tokens_in, gain_in, w0, w1, w2, w3, w4, w5, decay_in, gap_in, rgain_in, cgain_in, taps_in,
    out_r, out_c, o_ref, decay_v, gap_v, rgain_v, cgain_v, taps_v, tokens, gain,
    xs, x, wbuf, ow, pack, pk, lds, ld, dec, proj, gp, halo_s, halo_r, st_s, st_in, cacc, stat,
    yout, ya, mo, fin, ini, snd, w_own, w_recv, y_recv, d_recv, t_recv, p_recv, l_recv, h_recv,
    s_recv, c_recv, a_recv, o_own, o_recv, q_recv, g_recv, f_recv,
):
    s = lax.axis_index("sp")
    f = lax.axis_index("fs")
    t = lax.axis_index("tp")
    other = 1 - t
    col = lax.rem(f, 2)
    row = f // 2
    part = s // 2
    pair = lax.rem(s, 2)
    near = s + 1 - 2 * pair
    far = lax.rem(s + 2, 4)
    cross = 3 - s
    fx = f + 1 - 2 * col
    fy = lax.rem(f + 2, 4)
    fd = 3 - f
    head = 2 * pair + col
    rows = tokens.shape[1]
    span = 2 * rows
    total = 2 * span
    width = KD
    weights = (w0, w1, w2, w3, w4, w5)
    kslice = w0.shape[0]
    fourth = kslice // 4
    kinds = (range(4, 6), range(1, 4), range(0, 1))
    half = out_r.shape[0]
    quarter = half // 4
    cols = out_r.shape[1]
    groups = 4 * width
    ways = (near, 2 - part, 3 - 3 * part)
    NEAR, INNER, OUTER = range(3)
    mine = OUTER - (pair - part) * (pair - part)
    own_col = t == col
    own_weights = t == pair

    def at(sp=s, fs=f, tp=t):
        return {"sp": sp, "fs": fs, "tp": tp}

    def remote(src, dst, send, recv, to):
        return pltpu.make_async_remote_copy(
            src_ref=src, dst_ref=dst, send_sem=send, recv_sem=recv, device_id=to,
            device_id_type=MESH,
        )

    def when(cond, act):
        if cond is None:
            act()
        else:
            pl.when(cond)(act)

    def send(src, dst, group, recv, to, cond=None):
        when(cond, remote(src, dst, snd.at[group], recv, to).start)

    def arrived(ref, sem, cond=None):
        when(cond, pltpu.make_async_copy(ref, ref, sem).wait)

    def aligned(start, size, unit):
        return pl.ds(pl.multiple_of(start, unit), size)

    entry = [
        pltpu.make_async_copy(src, dst, ini.at[i])
        for i, (src, dst) in enumerate(
            (
                (tokens_in, tokens), (gain_in, gain), (decay_in, decay_v), (gap_in, gap_v),
                (rgain_in, rgain_v), (cgain_in, cgain_v), (taps_in, taps_v),
            )
        )
    ]
    for copy in entry:
        copy.start()

    def slot(place, core, k=None):
        if k is None:
            return aligned(place * span + core * rows, rows, rows)
        step = rows // TSUB
        return aligned(place * span + core * rows + k * step, step, step)

    barrier = pltpu.get_barrier_semaphore()
    greet = [at(sp=lax.rem(s + d, 4), tp=lax.rem(t + c, 2)) for d in range(4) for c in range(2) if d or c]
    greet += [at(sp=z, fs=fx, tp=lax.rem(t + c, 2)) for z in (s, near) for c in range(2)]
    greet += [at(fs=fy), at(fs=fd)]
    for to in greet:
        pl.semaphore_signal(barrier, inc=1, device_id=to, device_id_type=MESH)

    for copy in entry:
        copy.wait()
    values = tokens[0].astype(jnp.float32)
    normed = values * lax.rsqrt(jnp.mean(values * values, axis=-1, keepdims=True) + EPS)
    normed = (normed * gain[...]).astype(jnp.bfloat16)
    xs[...] = normed

    @pl.when(own_col)
    def _():
        x[slot(pair, t), :] = normed

    taps_n = taps_v.shape[0]
    at_col = aligned(col * width, width, width)
    pack[0:2, :] = gap_v[:, at_col]
    pack[2:3, :] = rgain_v[:, at_col]
    pack[3:4, :] = cgain_v[:, at_col]
    pack[4:PACK, :] = jnp.zeros((PACK - 4, width), jnp.float32)
    pack[PACK : PACK + taps_n, :] = taps_v[:, at_col].astype(jnp.float32)
    for j in range(2):
        lds[j, 0:2, :] = decay_v[0, :, j, :]
        lds[j, 2:PACK, :] = jnp.zeros((PACK - 2, span), jnp.float32)
    pl.semaphore_wait(barrier, len(greet))

    def piece(kind, place, side, core, i):
        size = fourth // PIECES[kind]
        at_cols = pl.ds(kinds[kind].start * width, len(kinds[kind]) * width)
        return wbuf.at[
            aligned(place * kslice + (side * 2 + core) * fourth + i * size, size, size), at_cols
        ]

    def flag(kind, way, i):
        return 3 * sum(PIECES[:kind]) + way * PIECES[kind] + i

    def send_weights(kind, i):
        size = fourth // PIECES[kind]
        for place, way in ((far, mine), (cross, mine), (near, NEAR)):
            for core in range(2):
                src_rows = aligned((row * 2 + core) * fourth + i * size, size, size)
                dst_rows = aligned(s * kslice + (row * 2 + core) * fourth + i * size, size, size)
                for m in kinds[kind]:
                    send(
                        weights[m].at[src_rows, at_col],
                        wbuf.at[dst_rows, pl.ds(m * width, width)],
                        WEIGHTS, w_recv.at[flag(kind, way, i)], at(sp=place, tp=core),
                        own_weights if place is far else jnp.logical_not(own_weights),
                    )

    @pl.when(own_weights)
    def _():
        pk[...] = pack[...]

    send(pack, pk, PARAMS, p_recv, at(tp=other), own_weights)
    for j in range(2):
        to = at(sp=2 * part + t, fs=2 * row + j, tp=col)
        here = own_weights & (col == j) & own_col

        @pl.when(here)
        def _(j=j):
            pltpu.make_async_copy(lds.at[j], ld.at[pair], l_recv.at[pair]).start()

        send(lds.at[j], ld.at[pair], DECAY + j, l_recv.at[pair], to, jnp.logical_not(here))

    def send_tokens(k):
        step = rows // TSUB
        src = xs.at[pl.ds(k * step, step)]
        dst = x.at[slot(pair, t, k)]
        sem = t_recv.at[pair, t, k]
        send(src, dst, TOKENS, sem, at(sp=near, tp=col))
        send(src, dst, TOKENS, sem, at(fs=fx, tp=col))
        send(src, dst, TOKENS_ON, sem, at(tp=col), jnp.logical_not(own_col))

    own_rows = aligned(s * kslice, kslice, kslice)
    for m in range(6):

        @pl.when(own_weights)
        def _(m=m):
            src = weights[m].at[:, at_col]
            dst = wbuf.at[own_rows, pl.ds(m * width, width)]
            kind = [m in k for k in kinds].index(True)
            remote(src, dst, snd.at[OWN], w_own.at[kind], at(tp=other)).start()
            pltpu.make_async_copy(src, dst, w_own.at[kind]).start()

    def out_cols(place):
        return aligned(place * cols, cols, cols)

    for which, ref in enumerate((out_r, out_c)):
        dst = ow.at[which, aligned(t * half, half, half), pl.ds(0, cols)]
        pltpu.make_async_copy(ref, dst, o_own.at[0]).start()
        send(ref, dst, OUT_OWN, o_own.at[1], at(tp=other))

    def relay_tokens(k):
        scope(f"T{k}")
        for core in range(2):
            ref = x.at[slot(1 - pair, core, k)]
            arrived(ref, t_recv.at[1 - pair, core, k], own_col)
            send(ref, ref, TOKENS_ON, t_recv.at[1 - pair, core, k], at(fs=fx), own_col)

    def first_hop(kind, way, i):
        scope(f"A{kind}{way}{i}")
        ref = piece(kind, ways[way], row, t, i)
        arrived(ref, w_recv.at[flag(kind, way, i)])
        send(ref, ref, ACROSS, y_recv.at[flag(kind, way, i)], at(fs=fy))
        send(ref, ref, BESIDE, d_recv.at[kind], at(tp=other))

    def second_hop(kind, way, i):
        scope(f"B{kind}{way}{i}")
        ref = piece(kind, ways[way], 1 - row, t, i)
        arrived(ref, y_recv.at[flag(kind, way, i)])
        send(ref, ref, BESIDE, d_recv.at[kind], at(tp=other))

    def weights_wait(kind):
        at_cols = pl.ds(kinds[kind].start * width, len(kinds[kind]) * width)
        arrived(wbuf.at[own_rows, at_cols], w_own.at[kind])
        arrived(wbuf.at[pl.ds(0, 6 * fourth), at_cols], d_recv.at[kind])

    cut = quarter // (OUTS // 2)

    def out_part(core, quart, k):
        return ow.at[
            k // (OUTS // 2),
            aligned(core * half + quart * quarter + k % (OUTS // 2) * cut, cut, cut),
            pl.ds(cols, cols),
        ]

    def send_out(k):
        src = (out_r, out_c)[k // (OUTS // 2)].at[
            aligned(f * quarter + k % (OUTS // 2) * cut, cut, cut), :
        ]
        send(src, out_part(t, f, k), OUT, o_recv.at[k], at(sp=far))

    def out_first(k):
        scope(f"X{k}")
        ref = out_part(t, f, k)
        arrived(ref, o_recv.at[k])
        send(ref, ref, OUT_ACROSS, q_recv.at[k, 0], at(fs=fx))
        send(ref, ref, OUT_ACROSS, q_recv.at[k, 1], at(fs=fy))
        send(ref, ref, OUT_BESIDE, g_recv, at(tp=other))

    def out_second(k):
        scope(f"Y{k}")
        for j, (source, to) in enumerate(((fx, fy), (fy, fx))):
            ref = out_part(t, source, k)
            arrived(ref, q_recv.at[k, j])
            if j == 0:
                send(ref, ref, OUT_ACROSS, q_recv.at[k, 2], at(fs=to))
            send(ref, ref, OUT_BESIDE, g_recv, at(tp=other))

    def out_third(k):
        scope(f"Z{k}")
        ref = out_part(t, fd, k)
        arrived(ref, q_recv.at[k, 2])
        send(ref, ref, OUT_BESIDE, g_recv, at(tp=other))

    def run(step, *pieces):
        for k in pieces:
            step(k)

    def project(kind):
        at_cols = pl.ds(kinds[kind].start * width, len(kinds[kind]) * width)
        proj[:, at_cols] = jnp.dot(
            x[...], wbuf[:, at_cols], preferred_element_type=jnp.float32
        ).astype(jnp.bfloat16)

    for k in range(TSUB):
        send_weights(0, k)
        send_tokens(k)
    for kind in range(1, 3):
        for i in range(PIECES[kind]):
            send_weights(kind, i)
    bf = jnp.bfloat16
    blocks = total // BLOCK
    pad = 16

    def decay_columns():
        scope("dec")
        for place in range(2):
            arrived(ld.at[place], l_recv.at[place])
        arrived(pk, p_recv, jnp.logical_not(own_weights))
        pick = lax.broadcasted_iota(jnp.int32, (PACK, width), 0)
        for place in range(2):
            for d in range(2):
                dec[d, pl.ds(place * span, span), :] = dot_as(
                    ld[place], (pick == d).astype(jnp.float32), 0, 0
                )

    def conv_open():
        scope("tokwait")
        for k in range(TSUB):
            for place in (pair, 1 - pair):
                for core in range(2):
                    local = own_col & (place == pair) & (t == core)
                    done = own_col & (place == 1 - pair)
                    skip = local | done if place is not pair else local
                    arrived(x.at[slot(place, core, k)], t_recv.at[place, core, k], jnp.logical_not(skip))
        scope("cwait")
        weights_wait(0)
        scope("projectc")
        project(0)
        scope("gate")
        conv_pre = proj[:, 4 * width : 5 * width].astype(jnp.float32)
        glu_pre = proj[:, 5 * width : 6 * width].astype(jnp.float32)
        gated = (conv_pre * jax.nn.sigmoid(glu_pre)).astype(jnp.bfloat16)
        gp[pad : pad + total, :] = gated.astype(jnp.float32)
        halo_s[...] = jnp.where(part == 0, gated[total - pad :], gated[0:pad])
        send(halo_s, halo_r, HALO, h_recv, at(sp=far))
        for k in range(OUTS):
            send_out(k)

    def conv_close():
        scope("conv")
        arrived(halo_r, h_recv)
        halo = halo_r[...].astype(jnp.float32)
        none = jnp.zeros((pad, width), jnp.float32)
        gp[0:pad, :] = jnp.where(part == 1, halo, none)
        gp[pad + total : 2 * pad + total, :] = jnp.where(part == 0, halo, none)
        first = pad - taps_n // 2
        for b in range(blocks):
            acc = jnp.zeros((BLOCK, width), jnp.float32)
            for j in range(taps_n):
                acc = acc + pk[PACK + j : PACK + j + 1, :] * gp[pl.ds(b * BLOCK + first + j, BLOCK), :]
            cacc[pl.ds(b * BLOCK, BLOCK), :] = acc
        conv = cacc[...]
        ones = jnp.ones((8, width), jnp.float32)
        stat[head, 0] = dot_as(ones, conv, 1, 1)
        stat[head, 1] = dot_as(ones, conv * conv, 1, 1)
        own_stat = stat.at[head]
        send(own_stat, own_stat, STATS, c_recv, at(fs=fx))
        send(own_stat, own_stat, STATS, c_recv, at(sp=near))
        send(own_stat, own_stat, STATS, c_recv, at(sp=near, fs=fx))

    order = [
        (0, INNER, 0), (0, NEAR, 0), (0, INNER, 1), (1, INNER, 0), (0, OUTER, 0), (0, NEAR, 1),
        (1, INNER, 1), (0, OUTER, 1), (1, INNER, 2), (1, OUTER, 0), (1, NEAR, 0), (1, INNER, 3),
        (1, OUTER, 1), (1, NEAR, 1), (1, OUTER, 2), (1, NEAR, 2), (1, OUTER, 3), (1, NEAR, 3),
        (2, INNER, 0), (2, OUTER, 0), (2, NEAR, 0),
    ]
    for k, hop in enumerate(order):
        if k == 4:
            relay_tokens(0)
        if k == 7:
            relay_tokens(1)
        first_hop(*hop)
        if k >= LAG:
            second_hop(*order[k - LAG])
        if k == 5:
            decay_columns()
        if k == 7 + LAG:
            conv_open()
    conv_close()
    for hop in order[-LAG:-3]:
        second_hop(*hop)
    scope("kwait")
    weights_wait(1)
    scope("projectk")
    project(1)

    scope("states")
    def f32(n0):
        return proj[:, n0 * width : (n0 + 1) * width].astype(jnp.float32)

    value = proj[:, width : 2 * width]
    keys, gates = [], []
    for d in range(2):
        key = pk[d : d + 1, :] * jax.nn.sigmoid(-f32(2 + d))
        keys.append(key)
        gates.append(jnp.log1p(-key) + dec[d])
    row_i = lax.broadcasted_iota(jnp.int32, (total, total), 0)
    col_i = lax.broadcasted_iota(jnp.int32, (total, total), 1)
    same = (row_i // BLOCK) == (col_i // BLOCK)
    lower = same & (row_i >= col_i)
    upper = same & (row_i <= col_i)
    both = jnp.concatenate(gates, axis=1)
    high = both.astype(bf)
    low = (both - high.astype(jnp.float32)).astype(bf)
    tri = lower.astype(jnp.float32).astype(bf)
    sums = jnp.dot(tri, high, preferred_element_type=jnp.float32) + jnp.dot(
        tri, low, preferred_element_type=jnp.float32
    )
    lasts = [sums[b * BLOCK + BLOCK - 1 : (b + 1) * BLOCK, :] for b in range(blocks)]

    def spread_rows(parts):
        return jnp.concatenate([jnp.broadcast_to(a, (BLOCK, width)) for a in parts], axis=0)

    last = [[a[:, d * width : (d + 1) * width] for a in lasts] for d in range(2)]
    last_rows = [spread_rows(last[d]) for d in range(2)]
    cum_f = sums[:, 0:width]
    cum_b = last_rows[1] - sums[:, width:] + gates[1]
    cums = (cum_f, cum_b)
    key_g = [(keys[d] * jnp.exp(-cums[d])).astype(bf) for d in range(2)]
    weighted = jnp.concatenate(
        [(keys[d] * jnp.exp(last_rows[d] - cums[d])).astype(bf) for d in range(2)], axis=1
    )
    outer = [
        lax.dot_general(
            value[b * BLOCK : (b + 1) * BLOCK], weighted[b * BLOCK : (b + 1) * BLOCK],
            (((0,), (0,)), ((), ())), preferred_element_type=jnp.float32,
        )
        for b in range(blocks)
    ]
    states = [[None] * blocks, [None] * blocks]
    ends, offsets = [], [[None] * blocks, [None] * blocks]
    for d in range(2):
        state = jnp.zeros((width, width), jnp.float32)
        offset = jnp.zeros((1, width), jnp.float32)
        for b in range(blocks) if d == 0 else range(blocks - 1, -1, -1):
            states[d][b] = state
            offsets[d][b] = offset
            state = state * jnp.exp(last[d][b]) + outer[b][:, d * width : (d + 1) * width]
            offset = offset + last[d][b]
        ends.append(state)
    st_s[...] = jnp.where(part == 0, ends[0], ends[1]).astype(bf)
    send(st_s, st_in, STATE, s_recv, at(sp=far))


    for hop in order[-3:]:
        second_hop(*hop)
    run(out_first, 0, 1, 2, 3)
    scope("qwait")
    weights_wait(2)
    scope("projectq")
    project(2)
    scope("scores")
    query_pre = f32(0)
    query = query_pre * jax.nn.sigmoid(query_pre) * width ** (-0.5)
    query_g = [(query * jnp.exp(cums[d])).astype(bf) for d in range(2)]
    scores = [
        lax.dot_general(
            query_g[d], key_g[d], (((1,), (1,)), ((), ())), preferred_element_type=jnp.float32
        )
        for d in range(2)
    ]
    scores = (jnp.where(lower, scores[0], 0.0) + jnp.where(upper, scores[1], 0.0)).astype(bf)
    inner = jnp.dot(scores, value, preferred_element_type=jnp.float32)
    carried = jnp.concatenate(
        [
            lax.dot_general(
                jnp.concatenate([q[b * BLOCK : (b + 1) * BLOCK] for q in query_g], axis=1),
                jnp.concatenate([states[d][b].astype(bf) for d in range(2)], axis=1),
                (((1,), (1,)), ((), ())), preferred_element_type=jnp.float32,
            )
            for b in range(blocks)
        ],
        axis=0,
    )
    reach = jnp.where(
        part == 1, spread_rows(offsets[0]) + cum_f, spread_rows(offsets[1]) + cum_b
    )
    query_in = (query * jnp.exp(reach)).astype(bf)
    def mix(which, out):
        for core in range(2):
            for place in range(2):
                at_row = place * span + core * rows
                yout[which, pl.ds(core * span + place * rows, rows), :] = out[
                    at_row : at_row + rows
                ].astype(bf)
        dst = ya.at[:, aligned(which * groups + head * width, width, width)]
        for place in (near, s):
            for core in range(2):
                src = yout.at[which, pl.ds(core * span, span)]
                here = own_col & (place == s) & (t == core)

                @pl.when(here)
                def _(src=src):
                    pltpu.make_async_copy(src, dst, a_recv.at[which]).start()

                send(
                    src, dst, MIXED, a_recv.at[which],
                    at(sp=place, fs=2 * row + t, tp=core), jnp.logical_not(here),
                )

    scope("statx")
    arrived(stat.at[pl.ds(0, 3)], c_recv)
    scope("cnorm")
    stats = (stat[0] + stat[1] + stat[2] + stat[3]) / groups
    mean_r = stats[0]
    inv_r = lax.rsqrt(stats[1] - mean_r * mean_r + EPS)
    eighth = jnp.full((8, width), 0.125, jnp.float32)
    mean_c = dot_as(mean_r, eighth, 0, 0)
    inv_c = dot_as(inv_r, eighth, 0, 0)
    out = (cacc[...] - mean_c) * inv_c * pk[3:4, :]
    mix(1, out * jax.nn.sigmoid(out))

    run(out_second, 0, 1)
    scope("statein")
    arrived(st_in, s_recv)
    scope("recnorm")
    joined = inner + carried + lax.dot_general(
        query_in, st_in[...], (((1,), (1,)), ((), ())), preferred_element_type=jnp.float32
    )
    joined = joined * lax.rsqrt(jnp.mean(joined * joined, axis=-1, keepdims=True) + EPS)
    mix(0, joined * pk[2:3, :])

    run(out_second, 2, 3)
    run(out_third, 0, 1, 2, 3)
    scope("ywait1")
    arrived(ya.at[:, pl.ds(0, groups)], a_recv.at[1])
    for k in range(2):
        arrived(ow.at[:, pl.ds(0, half), pl.ds(0, cols)], o_own.at[k])
    scope("ywait0")
    arrived(ya.at[:, pl.ds(0, groups)], a_recv.at[0])
    near_rows = aligned((1 - pair) * rows, rows, rows)
    for k in range(2):
        scope(f"outmm{k}")
        if k == 1:
            arrived(ow.at[:, pl.ds(0, half), pl.ds(0, cols)], g_recv)
        at_n = pl.ds(k * cols, cols)
        acc = jnp.dot(ya[:, 0:groups], ow[0, :, at_n], preferred_element_type=jnp.float32)
        acc = acc + jnp.dot(ya[:, groups:], ow[1, :, at_n], preferred_element_type=jnp.float32)
        mo[:, at_n] = acc.astype(bf)
        send(mo.at[near_rows, at_n], fin.at[:, at_n], GIVE, f_recv.at[k], at(sp=near))
    own_rows = aligned(pair * rows, rows, rows)
    for k, place in enumerate((s, far)):
        o_ref[0, :, out_cols(place)] = mo[own_rows, pl.ds(k * cols, cols)]
    for k, place in enumerate((near, cross)):
        scope(f"give{k}")
        at_n = pl.ds(k * cols, cols)
        arrived(fin.at[:, at_n], f_recv.at[k])
        o_ref[0, :, out_cols(place)] = fin[:, at_n]

    scope("sendwaits")
    other_weights = jnp.logical_not(own_weights)
    other_col = jnp.logical_not(own_col)
    arrived(pack, snd.at[PARAMS], own_weights)
    for j in range(2):
        here = own_weights & (col == j) & own_col
        arrived(lds.at[j], snd.at[DECAY + j], jnp.logical_not(here))
    arrived(x.at[pl.ds(0, 2 * rows)], snd.at[TOKENS])
    arrived(x.at[pl.ds(0, 2 * rows)], snd.at[TOKENS_ON], own_col)
    arrived(x.at[pl.ds(0, rows)], snd.at[TOKENS_ON], other_col)
    arrived(wbuf.at[pl.ds(0, 2 * fourth)], snd.at[WEIGHTS], own_weights)
    arrived(wbuf.at[pl.ds(0, 4 * fourth)], snd.at[WEIGHTS], other_weights)
    arrived(wbuf.at[pl.ds(0, kslice)], snd.at[OWN], own_weights)
    arrived(wbuf.at[pl.ds(0, 3 * fourth)], snd.at[ACROSS])
    arrived(wbuf.at[pl.ds(0, 6 * fourth)], snd.at[BESIDE])
    arrived(ow.at[:, pl.ds(0, half), pl.ds(0, cols)], snd.at[OUT_OWN])
    arrived(ow.at[:, pl.ds(0, quarter), pl.ds(0, cols)], snd.at[OUT])
    arrived(ow.at[:, pl.ds(0, 3 * quarter), pl.ds(0, cols)], snd.at[OUT_ACROSS])
    arrived(ow.at[:, pl.ds(0, 4 * quarter), pl.ds(0, cols)], snd.at[OUT_BESIDE])
    arrived(halo_s, snd.at[HALO])
    arrived(st_s, snd.at[STATE])
    arrived(stat.at[pl.ds(0, 3)], snd.at[STATS])
    arrived(x.at[pl.ds(0, 6 * span * width // x.shape[1])], snd.at[MIXED], own_col)
    arrived(x.at[pl.ds(0, 8 * span * width // x.shape[1])], snd.at[MIXED], other_col)
    arrived(fin, snd.at[GIVE])
    scope(None)


def scope(name):
    pass


def pair_body(
    tokens, norm_gain, rec_query, rec_input, rec_forward, rec_backward, forget_gap,
    log_decay, rec_gain, conv_value, conv_gate, conv_kernel, conv_gain, out_rec, out_conv,
):
    rows, d = tokens.shape[1:]
    total = 4 * rows
    taps = conv_kernel.shape[0]
    width = KD
    half, cols = out_rec.shape

    bf, f32 = jnp.bfloat16, jnp.float32
    dma = pltpu.SemaphoreType.DMA
    small = (log_decay, forget_gap, rec_gain[None], conv_gain[None], conv_kernel)
    scratch = [
        *(pltpu.VMEM(a.shape, a.dtype) for a in small),
        pltpu.VMEM(tokens.shape, bf),
        pltpu.VMEM((1, d), f32),
        pltpu.VMEM((rows, d), bf),
        pltpu.VMEM((total, d), bf),
        pltpu.VMEM((d, 6 * width), bf),
        pltpu.VMEM((2, 2 * half, 2 * cols), bf),
        pltpu.VMEM((PACK + taps, width), f32),
        pltpu.VMEM((PACK + taps, width), f32),
        pltpu.VMEM((2, PACK, 2 * rows), f32),
        pltpu.VMEM((2, PACK, 2 * rows), f32),
        pltpu.VMEM((2, total, width), f32),
        pltpu.VMEM((total, 6 * width), bf),
        pltpu.VMEM((total + 32, width), f32),
        pltpu.VMEM((16, width), bf),
        pltpu.VMEM((16, width), bf),
        pltpu.VMEM((width, width), bf),
        pltpu.VMEM((width, width), bf),
        pltpu.VMEM((total, width), f32),
        pltpu.VMEM((4, 2, 8, total), f32),
        pltpu.VMEM((2, total, width), bf),
        pltpu.VMEM((2 * rows, 8 * width), bf),
        pltpu.VMEM((2 * rows, 2 * cols), bf),
        pltpu.VMEM((rows, 2 * cols), bf),
        dma((7,)), dma((GROUPS,)), dma((3,)), dma((3 * sum(PIECES),)), dma((3 * sum(PIECES),)),
        dma((3,)), dma((2, 2, TSUB)), dma(()), dma((2,)), dma(()),
        dma(()), dma(()), dma((2,)), dma((2,)), dma((OUTS,)), dma((OUTS, 3)), dma(()), dma((2,)),
    ]
    return pl.pallas_call(
        pair_kernel,
        out_shape=pltpu.VMEM((1, rows, d), bf),
        in_specs=[pl.BlockSpec(memory_space=pl.ANY)] * 15,
        out_specs=pl.BlockSpec(memory_space=pltpu.VMEM),
        scratch_shapes=scratch,
        compiler_params=pltpu.CompilerParams(
            collective_id=0, has_side_effects=True, vmem_limit_bytes=60 * 1024 * 1024
        ),
    )(
        tokens, norm_gain[None], rec_query, rec_input, rec_forward, rec_backward, conv_value,
        conv_gate, *small, out_rec, out_conv,
    )


def fits(n, nf, nt, tokens, rec_query, log_decay, conv_value, conv_kernel, out_rec):
    heads = log_decay.shape[2]
    rows = tokens.shape[1] // (n * nt)
    return (
        nt == 2
        and n == 4
        and nf == 4
        and n == heads
        and tokens.shape[0] == nf
        and rec_query.shape[1] == heads * KD
        and conv_value.shape[1] == heads * VD
        and KD == VD
        and 2 * rows == KD
        and rows % (16 * TSUB) == 0
        and rec_query.shape[0] % (n * 4 * max(PIECES) * 16) == 0
        and out_rec.shape[0] % (nt * nf * 16) == 0
        and conv_kernel.shape[0] // 2 <= 15
    )


def layer(mesh, *args):
    n, nf, nt = (mesh.shape[a] for a in ("sp", "fs", "tp"))
    fast = fits(n, nf, nt, args[0], args[2], args[7], args[9], args[11], args[13])
    return sharded(mesh, pair_body if fast else body)(*args)


def solution(mesh):
    return functools.partial(layer, mesh)


def sharded(mesh, body):
    return jax.shard_map(
        body,
        mesh=mesh,
        in_specs=(
            P("fs", ("sp", "tp"), None),
            P(),
            P("sp", "tp"),
            P("sp", "tp"),
            P("sp", "tp"),
            P("sp", "tp"),
            P(None, "tp"),
            P("fs", None, "tp", "sp"),
            P("tp"),
            P("sp", "tp"),
            P("sp", "tp"),
            P(None, "tp"),
            P("tp"),
            P("tp", "sp"),
            P("tp", "sp"),
        ),
        out_specs=P("fs", ("sp", "tp"), None),
        check_vma=False,
    )
```

```python
import functools

import jax
import jax.numpy as jnp
from jax import lax
from jax.experimental import pallas as pl
from jax.experimental.pallas import tpu as pltpu
from jax.sharding import PartitionSpec as P

KD = 128
VD = 128
BLOCK = 64


EPS = 1e-06
HIGH = lax.Precision.HIGHEST


def entering(x, axis, join, neutral, backward):
    count = lax.axis_size(axis)
    place = lax.axis_index(axis)
    ahead = count - 1 - place if backward else place
    gathered = jax.tree.map(
        lambda a, kind: lax.all_gather(a.astype(kind), axis), x, (jnp.bfloat16, jnp.bfloat16)
    )
    state = jax.tree.map(lambda a, e: jnp.zeros_like(a) + jnp.asarray(e, a.dtype), x, neutral)

    def one(lap, state):
        source = count - 1 - lap if backward else lap
        return join(
            state,
            jax.tree.map(
                lambda a, own: lax.dynamic_index_in_dim(a, source, 0, False).astype(own.dtype),
                gathered,
                x,
            ),
        )

    return lax.fori_loop(0, ahead, one, state)


def padded_2(cells, sides, width):
    for axis, dim in sides:
        count = lax.axis_size(axis)
        ends = count - 1
        head = lax.slice_in_dim(cells, 0, width, axis=dim)
        tail = lax.slice_in_dim(cells, cells.shape[dim] - width, cells.shape[dim], axis=dim)
        cells = jnp.concatenate(
            [
                lax.ppermute(tail, axis, [(i, (i + 1) % count) for i in range(ends)]),
                cells,
                lax.ppermute(head, axis, [((i + 1) % count, i) for i in range(ends)]),
            ],
            axis=dim,
        )
    return cells


def block_pass(queries, key_rows, value_rows, log_gate):
    heads_n, length_n, key_dim = queries.shape
    value_dim = value_rows.shape[-1]
    blocks = length_n // BLOCK

    def split_blocks(tensor):
        return tensor.reshape(heads_n, blocks, BLOCK, tensor.shape[-1]).transpose(1, 0, 2, 3)

    def join_blocks(tensor):
        return tensor.transpose(1, 0, 2, 3).reshape(heads_n, length_n, tensor.shape[-1])

    lower_mask = jnp.tril(jnp.ones((BLOCK, BLOCK), bool))

    def advance(carried, inputs):
        states, offset = carried
        query_b, key_b, value_b, gate_b = inputs
        cumulative = jnp.cumsum(gate_b, axis=1)
        query_g = query_b * jnp.exp(cumulative)
        key_g = key_b * jnp.exp(-cumulative)
        scores = jnp.einsum("htd,hsd->hts", query_g, key_g, precision=HIGH)
        scores = jnp.where(lower_mask, scores, 0.0)
        result = jnp.einsum("hts,hse->hte", scores, value_b, precision=HIGH)
        result = result + jnp.einsum("htd,hde->hte", query_g, states, precision=HIGH)
        last_g = cumulative[:, -1, :]
        weighted = key_b * jnp.exp(last_g[:, None, :] - cumulative)
        states = jnp.exp(last_g)[:, :, None] * states + jnp.einsum(
            "hsd,hse->hde", weighted, value_b, precision=HIGH
        )
        decayed = query_b * jnp.exp(offset[:, None, :] + cumulative)
        return ((states, offset + last_g), (result, decayed))

    start_state = jnp.zeros((heads_n, key_dim, value_dim), jnp.float32)
    start_offset = jnp.zeros((heads_n, key_dim), jnp.float32)
    inputs = (
        split_blocks(queries),
        split_blocks(key_rows),
        split_blocks(value_rows),
        split_blocks(log_gate),
    )
    final_pair, outputs = lax.scan(advance, (start_state, start_offset), inputs)
    return (join_blocks(outputs[0]), join_blocks(outputs[1]), final_pair[1], final_pair[0])


def chain_combine(first_part, second_part):
    return (
        first_part[0] * second_part[0],
        second_part[0][:, :, None] * first_part[1] + second_part[1],
    )


def recurrence(query_pre, input_pre, forward_pre, backward_pre, forget_gap, log_decay, rec_gain):
    heads_local = log_decay.shape[2]
    row_count = query_pre.shape[0]

    def to_heads(tensor):
        return tensor.astype(jnp.float32).reshape(row_count, heads_local, -1).transpose(1, 0, 2)

    def gate_terms(pre_act, gap_row, decay_row):
        closing = jax.nn.sigmoid(-to_heads(pre_act)) * gap_row.reshape(heads_local, 1, -1)
        return (closing, jnp.log1p(-closing) + decay_row[:, :, None])

    queries = jax.nn.silu(to_heads(query_pre)) * KD ** (-0.5)
    values = to_heads(input_pre)
    keys_fwd, gate_fwd = gate_terms(forward_pre, forget_gap[0], log_decay[0, 0])
    keys_bwd, gate_bwd = gate_terms(backward_pre, forget_gap[1], log_decay[0, 1])
    identity = (
        jnp.ones((heads_local, KD), jnp.float32),
        jnp.zeros((heads_local, KD, VD), jnp.float32),
    )
    local_fwd, decayed_fwd, offset_fwd, state_fwd = block_pass(queries, keys_fwd, values, gate_fwd)
    incoming_fwd = entering((jnp.exp(offset_fwd), state_fwd), "sp", chain_combine, identity, False)
    forward = local_fwd + jnp.einsum("htd,hde->hte", decayed_fwd, incoming_fwd[1], precision=HIGH)
    local_bwd, decayed_bwd, offset_bwd, state_bwd = block_pass(
        jnp.flip(queries, 1), jnp.flip(keys_bwd, 1), jnp.flip(values, 1), jnp.flip(gate_bwd, 1)
    )
    incoming_bwd = entering((jnp.exp(offset_bwd), state_bwd), "sp", chain_combine, identity, True)
    backward = jnp.flip(
        local_bwd + jnp.einsum("htd,hde->hte", decayed_bwd, incoming_bwd[1], precision=HIGH), 1
    )
    joined = forward + backward
    joined = joined * lax.rsqrt(jnp.mean(joined * joined, axis=-1, keepdims=True) + EPS)
    joined = joined * rec_gain.reshape(heads_local, 1, VD)
    return joined.transpose(1, 0, 2).reshape(row_count, heads_local * VD).astype(jnp.bfloat16)


def convolve(conv_pre, glu_pre, conv_kernel, conv_gain):
    gated = (conv_pre.astype(jnp.float32) * jax.nn.sigmoid(glu_pre.astype(jnp.float32))).astype(
        jnp.bfloat16
    )
    half_width = conv_kernel.shape[0] // 2
    padded = padded_2(gated, (("sp", 0),), half_width)
    convolved = lax.conv_general_dilated(
        padded.astype(jnp.float32)[None],
        conv_kernel.astype(jnp.float32)[:, None, :],
        (1,),
        "VALID",
        dimension_numbers=("NWC", "WIO", "NWC"),
        feature_group_count=gated.shape[1],
        precision=HIGH,
    )[0]
    totals = lax.psum((jnp.sum(convolved, axis=-1), jnp.sum(convolved * convolved, axis=-1)), "tp")
    full_width = convolved.shape[1] * lax.axis_size("tp")
    mean_c = (totals[0] / full_width)[:, None]
    variance = (totals[1] / full_width)[:, None] - mean_c * mean_c
    return jax.nn.silu((convolved - mean_c) * lax.rsqrt(variance + EPS) * conv_gain).astype(
        jnp.bfloat16
    )


def body(
    tokens,
    norm_gain,
    rec_query,
    rec_input,
    rec_forward,
    rec_backward,
    forget_gap,
    log_decay,
    rec_gain,
    conv_value,
    conv_gate,
    conv_kernel,
    conv_gain,
    out_rec,
    out_conv,
):
    row_values = tokens[0].astype(jnp.float32)
    normed = row_values * lax.rsqrt(jnp.mean(row_values * row_values, axis=-1, keepdims=True) + EPS)
    normed = (normed * norm_gain).astype(jnp.bfloat16)
    whole = lax.all_gather(normed, "tp", axis=0, tiled=True)
    row_count = whole.shape[0]
    pieces = (
        lax.all_gather(rec_query, "sp", axis=0, tiled=True),
        lax.all_gather(rec_input, "sp", axis=0, tiled=True),
        lax.all_gather(rec_forward, "sp", axis=0, tiled=True),
        lax.all_gather(rec_backward, "sp", axis=0, tiled=True),
        lax.all_gather(conv_value, "sp", axis=0, tiled=True),
        lax.all_gather(conv_gate, "sp", axis=0, tiled=True),
    )
    results = tuple(
        (
            jnp.dot(whole, weight_piece, preferred_element_type=jnp.float32)
            for weight_piece in pieces
        )
    )
    projected = tuple((result.astype(jnp.bfloat16) for result in results))
    rec_out = recurrence(
        projected[0], projected[1], projected[2], projected[3], forget_gap, log_decay, rec_gain
    )
    conv_out = convolve(projected[4], projected[5], conv_kernel, conv_gain)
    both_out = jnp.concatenate([rec_out, conv_out], axis=1)
    out_local = jnp.concatenate([out_rec, out_conv], axis=0)
    full_columns = lax.all_gather(out_local, "sp", axis=1, tiled=True)
    own_rows = row_count // lax.axis_size("tp")
    rows_part = lax.slice_in_dim(both_out, 0, own_rows * lax.axis_size("tp"), axis=0)
    mixed = lax.psum_scatter(
        jnp.dot(rows_part, full_columns, preferred_element_type=jnp.float32).astype(jnp.bfloat16),
        "tp",
        scatter_dimension=0,
        tiled=True,
    )
    return mixed[None]


MESH = pl.DeviceIdType.MESH
PACK = 8


def dot_as(a, b, ca, cb, precision=HIGH):
    return lax.dot_general(
        a, b, (((ca,), (cb,)), ((), ())), precision=precision, preferred_element_type=jnp.float32
    )


PIECES = (2, 4, 1)
TSUB = 2
LAG = 6
OUTS = 4
OUT_AT = 15
(
    PARAMS, DECAY, _, TOKENS, TOKENS_ON, WEIGHTS, OWN, ACROSS, BESIDE, OUT_OWN, OUT, OUT_ACROSS,
    OUT_BESIDE, GIVE, HALO, STATE, STATS, MIXED, GROUPS,
) = range(19)


def pair_kernel(
    tokens_in, gain_in, w0, w1, w2, w3, w4, w5, decay_in, gap_in, rgain_in, cgain_in, taps_in,
    out_r, out_c, o_ref, decay_v, gap_v, rgain_v, cgain_v, taps_v, tokens, gain,
    xs, x, wbuf, ow, pack, pk, lds, ld, dec, proj, gp, halo_s, halo_r, st_s, st_in, cacc, stat,
    yout, ya, mo, fin, ini, snd, w_own, w_recv, y_recv, d_recv, t_recv, p_recv, l_recv, h_recv,
    s_recv, c_recv, a_recv, o_own, o_recv, q_recv, g_recv, f_recv,
):
    s = lax.axis_index("sp")
    f = lax.axis_index("fs")
    t = lax.axis_index("tp")
    other = 1 - t
    col = lax.rem(f, 2)
    row = f // 2
    part = s // 2
    pair = lax.rem(s, 2)
    near = s + 1 - 2 * pair
    far = lax.rem(s + 2, 4)
    cross = 3 - s
    fx = f + 1 - 2 * col
    fy = lax.rem(f + 2, 4)
    fd = 3 - f
    head = 2 * pair + col
    rows = tokens.shape[1]
    span = 2 * rows
    total = 2 * span
    width = KD
    weights = (w0, w1, w2, w3, w4, w5)
    kslice = w0.shape[0]
    fourth = kslice // 4
    kinds = (range(4, 6), range(1, 4), range(0, 1))
    half = out_r.shape[0]
    quarter = half // 4
    cols = out_r.shape[1]
    groups = 4 * width
    ways = (near, 2 - part, 3 - 3 * part)
    NEAR, INNER, OUTER = range(3)
    mine = OUTER - (pair - part) * (pair - part)
    own_col = t == col
    own_weights = t == pair

    def at(sp=s, fs=f, tp=t):
        return {"sp": sp, "fs": fs, "tp": tp}

    def remote(src, dst, send, recv, to):
        return pltpu.make_async_remote_copy(
            src_ref=src, dst_ref=dst, send_sem=send, recv_sem=recv, device_id=to,
            device_id_type=MESH,
        )

    def when(cond, act):
        if cond is None:
            act()
        else:
            pl.when(cond)(act)

    def send(src, dst, group, recv, to, cond=None):
        when(cond, remote(src, dst, snd.at[group], recv, to).start)

    def arrived(ref, sem, cond=None):
        when(cond, pltpu.make_async_copy(ref, ref, sem).wait)

    def aligned(start, size, unit):
        return pl.ds(pl.multiple_of(start, unit), size)

    entry = [
        pltpu.make_async_copy(src, dst, ini.at[i])
        for i, (src, dst) in enumerate(
            (
                (tokens_in, tokens), (gain_in, gain), (decay_in, decay_v), (gap_in, gap_v),
                (rgain_in, rgain_v), (cgain_in, cgain_v), (taps_in, taps_v),
            )
        )
    ]
    for copy in entry:
        copy.start()

    def slot(place, core, k=None):
        if k is None:
            return aligned(place * span + core * rows, rows, rows)
        step = rows // TSUB
        return aligned(place * span + core * rows + k * step, step, step)

    barrier = pltpu.get_barrier_semaphore()
    greet = [at(sp=lax.rem(s + d, 4), tp=lax.rem(t + c, 2)) for d in range(4) for c in range(2) if d or c]
    greet += [at(sp=z, fs=fx, tp=lax.rem(t + c, 2)) for z in (s, near) for c in range(2)]
    greet += [at(fs=fy), at(fs=fd)]
    for to in greet:
        pl.semaphore_signal(barrier, inc=1, device_id=to, device_id_type=MESH)

    for copy in entry:
        copy.wait()
    values = tokens[0].astype(jnp.float32)
    normed = values * lax.rsqrt(jnp.mean(values * values, axis=-1, keepdims=True) + EPS)
    normed = (normed * gain[...]).astype(jnp.bfloat16)
    xs[...] = normed

    @pl.when(own_col)
    def _():
        x[slot(pair, t), :] = normed

    taps_n = taps_v.shape[0]
    at_col = aligned(col * width, width, width)
    pack[0:2, :] = gap_v[:, at_col]
    pack[2:3, :] = rgain_v[:, at_col]
    pack[3:4, :] = cgain_v[:, at_col]
    pack[4:PACK, :] = jnp.zeros((PACK - 4, width), jnp.float32)
    pack[PACK : PACK + taps_n, :] = taps_v[:, at_col].astype(jnp.float32)
    for j in range(2):
        lds[j, 0:2, :] = decay_v[0, :, j, :]
        lds[j, 2:PACK, :] = jnp.zeros((PACK - 2, span), jnp.float32)
    pl.semaphore_wait(barrier, len(greet))

    def piece(kind, place, side, core, i):
        size = fourth // PIECES[kind]
        at_cols = pl.ds(kinds[kind].start * width, len(kinds[kind]) * width)
        return wbuf.at[
            aligned(place * kslice + (side * 2 + core) * fourth + i * size, size, size), at_cols
        ]

    def flag(kind, way, i):
        return 3 * sum(PIECES[:kind]) + way * PIECES[kind] + i

    def send_weights(kind, i):
        size = fourth // PIECES[kind]
        for place, way in ((far, mine), (cross, mine), (near, NEAR)):
            for core in range(2):
                src_rows = aligned((row * 2 + core) * fourth + i * size, size, size)
                dst_rows = aligned(s * kslice + (row * 2 + core) * fourth + i * size, size, size)
                for m in kinds[kind]:
                    send(
                        weights[m].at[src_rows, at_col],
                        wbuf.at[dst_rows, pl.ds(m * width, width)],
                        WEIGHTS, w_recv.at[flag(kind, way, i)], at(sp=place, tp=core),
                        own_weights if place is far else jnp.logical_not(own_weights),
                    )

    @pl.when(own_weights)
    def _():
        pk[...] = pack[...]

    send(pack, pk, PARAMS, p_recv, at(tp=other), own_weights)
    for j in range(2):
        to = at(sp=2 * part + t, fs=2 * row + j, tp=col)
        here = own_weights & (col == j) & own_col

        @pl.when(here)
        def _(j=j):
            pltpu.make_async_copy(lds.at[j], ld.at[pair], l_recv.at[pair]).start()

        send(lds.at[j], ld.at[pair], DECAY + j, l_recv.at[pair], to, jnp.logical_not(here))

    def send_tokens(k):
        step = rows // TSUB
        src = xs.at[pl.ds(k * step, step)]
        dst = x.at[slot(pair, t, k)]
        sem = t_recv.at[pair, t, k]
        send(src, dst, TOKENS, sem, at(sp=near, tp=col))
        send(src, dst, TOKENS, sem, at(fs=fx, tp=col))
        send(src, dst, TOKENS_ON, sem, at(tp=col), jnp.logical_not(own_col))

    own_rows = aligned(s * kslice, kslice, kslice)
    for m in range(6):

        @pl.when(own_weights)
        def _(m=m):
            src = weights[m].at[:, at_col]
            dst = wbuf.at[own_rows, pl.ds(m * width, width)]
            kind = [m in k for k in kinds].index(True)
            remote(src, dst, snd.at[OWN], w_own.at[kind], at(tp=other)).start()
            pltpu.make_async_copy(src, dst, w_own.at[kind]).start()

    def out_cols(place):
        return aligned(place * cols, cols, cols)

    for which, ref in enumerate((out_r, out_c)):
        dst = ow.at[which, aligned(t * half, half, half), pl.ds(0, cols)]
        pltpu.make_async_copy(ref, dst, o_own.at[0]).start()
        send(ref, dst, OUT_OWN, o_own.at[1], at(tp=other))

    def relay_tokens(k):
        scope(f"T{k}")
        for core in range(2):
            ref = x.at[slot(1 - pair, core, k)]
            arrived(ref, t_recv.at[1 - pair, core, k], own_col)
            send(ref, ref, TOKENS_ON, t_recv.at[1 - pair, core, k], at(fs=fx), own_col)

    def first_hop(kind, way, i):
        scope(f"A{kind}{way}{i}")
        ref = piece(kind, ways[way], row, t, i)
        arrived(ref, w_recv.at[flag(kind, way, i)])
        send(ref, ref, ACROSS, y_recv.at[flag(kind, way, i)], at(fs=fy))
        send(ref, ref, BESIDE, d_recv.at[kind], at(tp=other))

    def second_hop(kind, way, i):
        scope(f"B{kind}{way}{i}")
        ref = piece(kind, ways[way], 1 - row, t, i)
        arrived(ref, y_recv.at[flag(kind, way, i)])
        send(ref, ref, BESIDE, d_recv.at[kind], at(tp=other))

    def weights_wait(kind):
        at_cols = pl.ds(kinds[kind].start * width, len(kinds[kind]) * width)
        arrived(wbuf.at[own_rows, at_cols], w_own.at[kind])
        arrived(wbuf.at[pl.ds(0, 6 * fourth), at_cols], d_recv.at[kind])

    cut = quarter // (OUTS // 2)

    def out_part(core, quart, k):
        return ow.at[
            k // (OUTS // 2),
            aligned(core * half + quart * quarter + k % (OUTS // 2) * cut, cut, cut),
            pl.ds(cols, cols),
        ]

    def send_out(k):
        src = (out_r, out_c)[k // (OUTS // 2)].at[
            aligned(f * quarter + k % (OUTS // 2) * cut, cut, cut), :
        ]
        send(src, out_part(t, f, k), OUT, o_recv.at[k], at(sp=far))

    def out_first(k):
        scope(f"X{k}")
        ref = out_part(t, f, k)
        arrived(ref, o_recv.at[k])
        send(ref, ref, OUT_ACROSS, q_recv.at[k, 0], at(fs=fx))
        send(ref, ref, OUT_ACROSS, q_recv.at[k, 1], at(fs=fy))
        send(ref, ref, OUT_BESIDE, g_recv, at(tp=other))

    def out_second(k):
        scope(f"Y{k}")
        for j, (source, to) in enumerate(((fx, fy), (fy, fx))):
            ref = out_part(t, source, k)
            arrived(ref, q_recv.at[k, j])
            if j == 0:
                send(ref, ref, OUT_ACROSS, q_recv.at[k, 2], at(fs=to))
            send(ref, ref, OUT_BESIDE, g_recv, at(tp=other))

    def out_third(k):
        scope(f"Z{k}")
        ref = out_part(t, fd, k)
        arrived(ref, q_recv.at[k, 2])
        send(ref, ref, OUT_BESIDE, g_recv, at(tp=other))

    def run(step, *pieces):
        for k in pieces:
            step(k)

    def project(kind):
        at_cols = pl.ds(kinds[kind].start * width, len(kinds[kind]) * width)
        proj[:, at_cols] = jnp.dot(
            x[...], wbuf[:, at_cols], preferred_element_type=jnp.float32
        ).astype(jnp.bfloat16)

    for k in range(TSUB):
        send_weights(0, k)
        send_tokens(k)
    for kind in range(1, 3):
        for i in range(PIECES[kind]):
            send_weights(kind, i)
    bf = jnp.bfloat16
    blocks = total // BLOCK
    pad = 16

    def decay_columns():
        scope("dec")
        for place in range(2):
            arrived(ld.at[place], l_recv.at[place])
        arrived(pk, p_recv, jnp.logical_not(own_weights))
        pick = lax.broadcasted_iota(jnp.int32, (PACK, width), 0)
        for place in range(2):
            for d in range(2):
                dec[d, pl.ds(place * span, span), :] = dot_as(
                    ld[place], (pick == d).astype(jnp.float32), 0, 0
                )

    def conv_open():
        scope("tokwait")
        for k in range(TSUB):
            for place in (pair, 1 - pair):
                for core in range(2):
                    local = own_col & (place == pair) & (t == core)
                    done = own_col & (place == 1 - pair)
                    skip = local | done if place is not pair else local
                    arrived(x.at[slot(place, core, k)], t_recv.at[place, core, k], jnp.logical_not(skip))
        scope("cwait")
        weights_wait(0)
        scope("projectc")
        project(0)
        scope("gate")
        conv_pre = proj[:, 4 * width : 5 * width].astype(jnp.float32)
        glu_pre = proj[:, 5 * width : 6 * width].astype(jnp.float32)
        gated = (conv_pre * jax.nn.sigmoid(glu_pre)).astype(jnp.bfloat16)
        gp[pad : pad + total, :] = gated.astype(jnp.float32)
        halo_s[...] = jnp.where(part == 0, gated[total - pad :], gated[0:pad])
        send(halo_s, halo_r, HALO, h_recv, at(sp=far))
        for k in range(OUTS // 2, OUTS):
            send_out(k)

    def conv_close():
        scope("conv")
        arrived(halo_r, h_recv)
        halo = halo_r[...].astype(jnp.float32)
        none = jnp.zeros((pad, width), jnp.float32)
        gp[0:pad, :] = jnp.where(part == 1, halo, none)
        gp[pad + total : 2 * pad + total, :] = jnp.where(part == 0, halo, none)
        first = pad - taps_n // 2
        for b in range(blocks):
            acc = jnp.zeros((BLOCK, width), jnp.float32)
            for j in range(taps_n):
                acc = acc + pk[PACK + j : PACK + j + 1, :] * gp[pl.ds(b * BLOCK + first + j, BLOCK), :]
            cacc[pl.ds(b * BLOCK, BLOCK), :] = acc
        conv = cacc[...]
        ones = jnp.ones((8, width), jnp.float32)
        stat[head, 0] = dot_as(ones, conv, 1, 1)
        stat[head, 1] = dot_as(ones, conv * conv, 1, 1)
        own_stat = stat.at[head]
        send(own_stat, own_stat, STATS, c_recv, at(fs=fx))
        send(own_stat, own_stat, STATS, c_recv, at(sp=near))
        send(own_stat, own_stat, STATS, c_recv, at(sp=near, fs=fx))

    order = [
        (0, INNER, 0), (0, NEAR, 0), (0, INNER, 1), (1, INNER, 0), (0, OUTER, 0), (0, NEAR, 1),
        (1, INNER, 1), (0, OUTER, 1), (1, INNER, 2), (1, OUTER, 0), (1, NEAR, 0), (1, INNER, 3),
        (1, OUTER, 1), (1, NEAR, 1), (1, OUTER, 2), (1, NEAR, 2), (1, OUTER, 3), (1, NEAR, 3),
        (2, INNER, 0), (2, OUTER, 0), (2, NEAR, 0),
    ]
    for k, hop in enumerate(order):
        if k == 4:
            relay_tokens(0)
        if k == 7:
            relay_tokens(1)
        first_hop(*hop)
        if k >= LAG:
            second_hop(*order[k - LAG])
        if k == 5:
            decay_columns()
        if k == OUT_AT:
            for early in range(OUTS // 2):
                send_out(early)
        if k == 17:
            conv_open()
    for hop in order[-LAG:-3]:
        second_hop(*hop)
    scope("kwait")
    weights_wait(1)
    scope("projectk")
    project(1)

    scope("states")
    def f32(n0):
        return proj[:, n0 * width : (n0 + 1) * width].astype(jnp.float32)

    value = proj[:, width : 2 * width]
    keys, gates = [], []
    for d in range(2):
        key = pk[d : d + 1, :] * jax.nn.sigmoid(-f32(2 + d))
        keys.append(key)
        gates.append(jnp.log1p(-key) + dec[d])
    row_i = lax.broadcasted_iota(jnp.int32, (total, total), 0)
    col_i = lax.broadcasted_iota(jnp.int32, (total, total), 1)
    same = (row_i // BLOCK) == (col_i // BLOCK)
    lower = same & (row_i >= col_i)
    upper = same & (row_i <= col_i)
    both = jnp.concatenate(gates, axis=1)
    high = both.astype(bf)
    low = (both - high.astype(jnp.float32)).astype(bf)
    tri = lower.astype(jnp.float32).astype(bf)
    sums = jnp.dot(tri, high, preferred_element_type=jnp.float32) + jnp.dot(
        tri, low, preferred_element_type=jnp.float32
    )
    lasts = [sums[b * BLOCK + BLOCK - 1 : (b + 1) * BLOCK, :] for b in range(blocks)]

    def spread_rows(parts):
        return jnp.concatenate([jnp.broadcast_to(a, (BLOCK, width)) for a in parts], axis=0)

    last = [[a[:, d * width : (d + 1) * width] for a in lasts] for d in range(2)]
    last_rows = [spread_rows(last[d]) for d in range(2)]
    cum_f = sums[:, 0:width]
    cum_b = last_rows[1] - sums[:, width:] + gates[1]
    cums = (cum_f, cum_b)
    key_g = [(keys[d] * jnp.exp(-cums[d])).astype(bf) for d in range(2)]
    weighted = jnp.concatenate(
        [(keys[d] * jnp.exp(last_rows[d] - cums[d])).astype(bf) for d in range(2)], axis=1
    )
    outer = [
        lax.dot_general(
            value[b * BLOCK : (b + 1) * BLOCK], weighted[b * BLOCK : (b + 1) * BLOCK],
            (((0,), (0,)), ((), ())), preferred_element_type=jnp.float32,
        )
        for b in range(blocks)
    ]
    states = [[None] * blocks, [None] * blocks]
    ends, offsets = [], [[None] * blocks, [None] * blocks]
    for d in range(2):
        state = jnp.zeros((width, width), jnp.float32)
        offset = jnp.zeros((1, width), jnp.float32)
        for b in range(blocks) if d == 0 else range(blocks - 1, -1, -1):
            states[d][b] = state
            offsets[d][b] = offset
            state = state * jnp.exp(last[d][b]) + outer[b][:, d * width : (d + 1) * width]
            offset = offset + last[d][b]
        ends.append(state)
    st_s[...] = jnp.where(part == 0, ends[0], ends[1]).astype(bf)
    send(st_s, st_in, STATE, s_recv, at(sp=far))


    for hop in order[-3:]:
        second_hop(*hop)
    run(out_first, 0, 1)
    conv_close()
    scope("qwait")
    weights_wait(2)
    scope("projectq")
    project(2)
    scope("scores")
    query_pre = f32(0)
    query = query_pre * jax.nn.sigmoid(query_pre) * width ** (-0.5)
    query_g = [(query * jnp.exp(cums[d])).astype(bf) for d in range(2)]
    scores = [
        lax.dot_general(
            query_g[d], key_g[d], (((1,), (1,)), ((), ())), preferred_element_type=jnp.float32
        )
        for d in range(2)
    ]
    scores = (jnp.where(lower, scores[0], 0.0) + jnp.where(upper, scores[1], 0.0)).astype(bf)
    inner = jnp.dot(scores, value, preferred_element_type=jnp.float32)
    carried = jnp.concatenate(
        [
            lax.dot_general(
                jnp.concatenate([q[b * BLOCK : (b + 1) * BLOCK] for q in query_g], axis=1),
                jnp.concatenate([states[d][b].astype(bf) for d in range(2)], axis=1),
                (((1,), (1,)), ((), ())), preferred_element_type=jnp.float32,
            )
            for b in range(blocks)
        ],
        axis=0,
    )
    reach = jnp.where(
        part == 1, spread_rows(offsets[0]) + cum_f, spread_rows(offsets[1]) + cum_b
    )
    query_in = (query * jnp.exp(reach)).astype(bf)
    def mix(which, out):
        for core in range(2):
            for place in range(2):
                at_row = place * span + core * rows
                yout[which, pl.ds(core * span + place * rows, rows), :] = out[
                    at_row : at_row + rows
                ].astype(bf)
        dst = ya.at[:, aligned(which * groups + head * width, width, width)]
        for place in (near, s):
            for core in range(2):
                src = yout.at[which, pl.ds(core * span, span)]
                here = own_col & (place == s) & (t == core)

                @pl.when(here)
                def _(src=src):
                    pltpu.make_async_copy(src, dst, a_recv.at[which]).start()

                send(
                    src, dst, MIXED, a_recv.at[which],
                    at(sp=place, fs=2 * row + t, tp=core), jnp.logical_not(here),
                )

    run(out_first, 2, 3)
    scope("statein")
    arrived(st_in, s_recv)
    scope("recnorm")
    joined = inner + carried + lax.dot_general(
        query_in, st_in[...], (((1,), (1,)), ((), ())), preferred_element_type=jnp.float32
    )
    joined = joined * lax.rsqrt(jnp.mean(joined * joined, axis=-1, keepdims=True) + EPS)
    mix(0, joined * pk[2:3, :])

    run(out_second, 0, 1)
    scope("statx")
    arrived(stat.at[pl.ds(0, 3)], c_recv)
    scope("cnorm")
    stats = (stat[0] + stat[1] + stat[2] + stat[3]) / groups
    mean_r = stats[0]
    inv_r = lax.rsqrt(stats[1] - mean_r * mean_r + EPS)
    eighth = jnp.full((8, width), 0.125, jnp.float32)
    mean_c = dot_as(mean_r, eighth, 0, 0)
    inv_c = dot_as(inv_r, eighth, 0, 0)
    out = (cacc[...] - mean_c) * inv_c * pk[3:4, :]
    mix(1, out * jax.nn.sigmoid(out))

    run(out_second, 2, 3)
    run(out_third, 0, 1, 2, 3)
    scope("ywait1")
    arrived(ya.at[:, pl.ds(0, groups)], a_recv.at[1])
    for k in range(2):
        arrived(ow.at[:, pl.ds(0, half), pl.ds(0, cols)], o_own.at[k])
    scope("ywait0")
    arrived(ya.at[:, pl.ds(0, groups)], a_recv.at[0])
    near_rows = aligned((1 - pair) * rows, rows, rows)
    for k in range(2):
        scope(f"outmm{k}")
        if k == 1:
            arrived(ow.at[:, pl.ds(0, half), pl.ds(0, cols)], g_recv)
        at_n = pl.ds(k * cols, cols)
        acc = jnp.dot(ya[:, 0:groups], ow[0, :, at_n], preferred_element_type=jnp.float32)
        acc = acc + jnp.dot(ya[:, groups:], ow[1, :, at_n], preferred_element_type=jnp.float32)
        mo[:, at_n] = acc.astype(bf)
        send(mo.at[near_rows, at_n], fin.at[:, at_n], GIVE, f_recv.at[k], at(sp=near))
    own_rows = aligned(pair * rows, rows, rows)
    for k, place in enumerate((s, far)):
        o_ref[0, :, out_cols(place)] = mo[own_rows, pl.ds(k * cols, cols)]
    for k, place in enumerate((near, cross)):
        scope(f"give{k}")
        at_n = pl.ds(k * cols, cols)
        arrived(fin.at[:, at_n], f_recv.at[k])
        o_ref[0, :, out_cols(place)] = fin[:, at_n]

    scope("sendwaits")
    other_weights = jnp.logical_not(own_weights)
    other_col = jnp.logical_not(own_col)
    arrived(pack, snd.at[PARAMS], own_weights)
    for j in range(2):
        here = own_weights & (col == j) & own_col
        arrived(lds.at[j], snd.at[DECAY + j], jnp.logical_not(here))
    arrived(x.at[pl.ds(0, 2 * rows)], snd.at[TOKENS])
    arrived(x.at[pl.ds(0, 2 * rows)], snd.at[TOKENS_ON], own_col)
    arrived(x.at[pl.ds(0, rows)], snd.at[TOKENS_ON], other_col)
    arrived(wbuf.at[pl.ds(0, 2 * fourth)], snd.at[WEIGHTS], own_weights)
    arrived(wbuf.at[pl.ds(0, 4 * fourth)], snd.at[WEIGHTS], other_weights)
    arrived(wbuf.at[pl.ds(0, kslice)], snd.at[OWN], own_weights)
    arrived(wbuf.at[pl.ds(0, 3 * fourth)], snd.at[ACROSS])
    arrived(wbuf.at[pl.ds(0, 6 * fourth)], snd.at[BESIDE])
    arrived(ow.at[:, pl.ds(0, half), pl.ds(0, cols)], snd.at[OUT_OWN])
    arrived(ow.at[:, pl.ds(0, quarter), pl.ds(0, cols)], snd.at[OUT])
    arrived(ow.at[:, pl.ds(0, 3 * quarter), pl.ds(0, cols)], snd.at[OUT_ACROSS])
    arrived(ow.at[:, pl.ds(0, 4 * quarter), pl.ds(0, cols)], snd.at[OUT_BESIDE])
    arrived(halo_s, snd.at[HALO])
    arrived(st_s, snd.at[STATE])
    arrived(stat.at[pl.ds(0, 3)], snd.at[STATS])
    arrived(x.at[pl.ds(0, 6 * span * width // x.shape[1])], snd.at[MIXED], own_col)
    arrived(x.at[pl.ds(0, 8 * span * width // x.shape[1])], snd.at[MIXED], other_col)
    arrived(fin, snd.at[GIVE])
    scope(None)


def scope(name):
    pass


def pair_body(
    tokens, norm_gain, rec_query, rec_input, rec_forward, rec_backward, forget_gap,
    log_decay, rec_gain, conv_value, conv_gate, conv_kernel, conv_gain, out_rec, out_conv,
):
    rows, d = tokens.shape[1:]
    total = 4 * rows
    taps = conv_kernel.shape[0]
    width = KD
    half, cols = out_rec.shape

    bf, f32 = jnp.bfloat16, jnp.float32
    dma = pltpu.SemaphoreType.DMA
    small = (log_decay, forget_gap, rec_gain[None], conv_gain[None], conv_kernel)
    scratch = [
        *(pltpu.VMEM(a.shape, a.dtype) for a in small),
        pltpu.VMEM(tokens.shape, bf),
        pltpu.VMEM((1, d), f32),
        pltpu.VMEM((rows, d), bf),
        pltpu.VMEM((total, d), bf),
        pltpu.VMEM((d, 6 * width), bf),
        pltpu.VMEM((2, 2 * half, 2 * cols), bf),
        pltpu.VMEM((PACK + taps, width), f32),
        pltpu.VMEM((PACK + taps, width), f32),
        pltpu.VMEM((2, PACK, 2 * rows), f32),
        pltpu.VMEM((2, PACK, 2 * rows), f32),
        pltpu.VMEM((2, total, width), f32),
        pltpu.VMEM((total, 6 * width), bf),
        pltpu.VMEM((total + 32, width), f32),
        pltpu.VMEM((16, width), bf),
        pltpu.VMEM((16, width), bf),
        pltpu.VMEM((width, width), bf),
        pltpu.VMEM((width, width), bf),
        pltpu.VMEM((total, width), f32),
        pltpu.VMEM((4, 2, 8, total), f32),
        pltpu.VMEM((2, total, width), bf),
        pltpu.VMEM((2 * rows, 8 * width), bf),
        pltpu.VMEM((2 * rows, 2 * cols), bf),
        pltpu.VMEM((rows, 2 * cols), bf),
        dma((7,)), dma((GROUPS,)), dma((3,)), dma((3 * sum(PIECES),)), dma((3 * sum(PIECES),)),
        dma((3,)), dma((2, 2, TSUB)), dma(()), dma((2,)), dma(()),
        dma(()), dma(()), dma((2,)), dma((2,)), dma((OUTS,)), dma((OUTS, 3)), dma(()), dma((2,)),
    ]
    return pl.pallas_call(
        pair_kernel,
        out_shape=pltpu.VMEM((1, rows, d), bf),
        in_specs=[pl.BlockSpec(memory_space=pl.ANY)] * 15,
        out_specs=pl.BlockSpec(memory_space=pltpu.VMEM),
        scratch_shapes=scratch,
        compiler_params=pltpu.CompilerParams(
            collective_id=0, has_side_effects=True, vmem_limit_bytes=60 * 1024 * 1024
        ),
    )(
        tokens, norm_gain[None], rec_query, rec_input, rec_forward, rec_backward, conv_value,
        conv_gate, *small, out_rec, out_conv,
    )


def fits(n, nf, nt, tokens, rec_query, log_decay, conv_value, conv_kernel, out_rec):
    heads = log_decay.shape[2]
    rows = tokens.shape[1] // (n * nt)
    return (
        nt == 2
        and n == 4
        and nf == 4
        and n == heads
        and tokens.shape[0] == nf
        and rec_query.shape[1] == heads * KD
        and conv_value.shape[1] == heads * VD
        and KD == VD
        and 2 * rows == KD
        and rows % (16 * TSUB) == 0
        and rec_query.shape[0] % (n * 4 * max(PIECES) * 16) == 0
        and out_rec.shape[0] % (nt * nf * 16) == 0
        and conv_kernel.shape[0] // 2 <= 15
    )


def layer(mesh, *args):
    n, nf, nt = (mesh.shape[a] for a in ("sp", "fs", "tp"))
    fast = fits(n, nf, nt, args[0], args[2], args[7], args[9], args[11], args[13])
    return sharded(mesh, pair_body if fast else body)(*args)


def solution(mesh):
    return functools.partial(layer, mesh)


def sharded(mesh, body):
    return jax.shard_map(
        body,
        mesh=mesh,
        in_specs=(
            P("fs", ("sp", "tp"), None),
            P(),
            P("sp", "tp"),
            P("sp", "tp"),
            P("sp", "tp"),
            P("sp", "tp"),
            P(None, "tp"),
            P("fs", None, "tp", "sp"),
            P("tp"),
            P("sp", "tp"),
            P("sp", "tp"),
            P(None, "tp"),
            P("tp"),
            P("tp", "sp"),
            P("tp", "sp"),
        ),
        out_specs=P("fs", ("sp", "tp"), None),
        check_vma=False,
    )
```

```python
import functools

import jax
import jax.numpy as jnp
from jax import lax
from jax.experimental import pallas as pl
from jax.experimental.pallas import tpu as pltpu
from jax.sharding import PartitionSpec as P

KD = 128
VD = 128
BLOCK = 64


EPS = 1e-06
HIGH = lax.Precision.HIGHEST


def entering(x, axis, join, neutral, backward):
    count = lax.axis_size(axis)
    place = lax.axis_index(axis)
    ahead = count - 1 - place if backward else place
    gathered = jax.tree.map(
        lambda a, kind: lax.all_gather(a.astype(kind), axis), x, (jnp.bfloat16, jnp.bfloat16)
    )
    state = jax.tree.map(lambda a, e: jnp.zeros_like(a) + jnp.asarray(e, a.dtype), x, neutral)

    def one(lap, state):
        source = count - 1 - lap if backward else lap
        return join(
            state,
            jax.tree.map(
                lambda a, own: lax.dynamic_index_in_dim(a, source, 0, False).astype(own.dtype),
                gathered,
                x,
            ),
        )

    return lax.fori_loop(0, ahead, one, state)


def padded_2(cells, sides, width):
    for axis, dim in sides:
        count = lax.axis_size(axis)
        ends = count - 1
        head = lax.slice_in_dim(cells, 0, width, axis=dim)
        tail = lax.slice_in_dim(cells, cells.shape[dim] - width, cells.shape[dim], axis=dim)
        cells = jnp.concatenate(
            [
                lax.ppermute(tail, axis, [(i, (i + 1) % count) for i in range(ends)]),
                cells,
                lax.ppermute(head, axis, [((i + 1) % count, i) for i in range(ends)]),
            ],
            axis=dim,
        )
    return cells


def block_pass(queries, key_rows, value_rows, log_gate):
    heads_n, length_n, key_dim = queries.shape
    value_dim = value_rows.shape[-1]
    blocks = length_n // BLOCK

    def split_blocks(tensor):
        return tensor.reshape(heads_n, blocks, BLOCK, tensor.shape[-1]).transpose(1, 0, 2, 3)

    def join_blocks(tensor):
        return tensor.transpose(1, 0, 2, 3).reshape(heads_n, length_n, tensor.shape[-1])

    lower_mask = jnp.tril(jnp.ones((BLOCK, BLOCK), bool))

    def advance(carried, inputs):
        states, offset = carried
        query_b, key_b, value_b, gate_b = inputs
        cumulative = jnp.cumsum(gate_b, axis=1)
        query_g = query_b * jnp.exp(cumulative)
        key_g = key_b * jnp.exp(-cumulative)
        scores = jnp.einsum("htd,hsd->hts", query_g, key_g, precision=HIGH)
        scores = jnp.where(lower_mask, scores, 0.0)
        result = jnp.einsum("hts,hse->hte", scores, value_b, precision=HIGH)
        result = result + jnp.einsum("htd,hde->hte", query_g, states, precision=HIGH)
        last_g = cumulative[:, -1, :]
        weighted = key_b * jnp.exp(last_g[:, None, :] - cumulative)
        states = jnp.exp(last_g)[:, :, None] * states + jnp.einsum(
            "hsd,hse->hde", weighted, value_b, precision=HIGH
        )
        decayed = query_b * jnp.exp(offset[:, None, :] + cumulative)
        return ((states, offset + last_g), (result, decayed))

    start_state = jnp.zeros((heads_n, key_dim, value_dim), jnp.float32)
    start_offset = jnp.zeros((heads_n, key_dim), jnp.float32)
    inputs = (
        split_blocks(queries),
        split_blocks(key_rows),
        split_blocks(value_rows),
        split_blocks(log_gate),
    )
    final_pair, outputs = lax.scan(advance, (start_state, start_offset), inputs)
    return (join_blocks(outputs[0]), join_blocks(outputs[1]), final_pair[1], final_pair[0])


def chain_combine(first_part, second_part):
    return (
        first_part[0] * second_part[0],
        second_part[0][:, :, None] * first_part[1] + second_part[1],
    )


def recurrence(query_pre, input_pre, forward_pre, backward_pre, forget_gap, log_decay, rec_gain):
    heads_local = log_decay.shape[2]
    row_count = query_pre.shape[0]

    def to_heads(tensor):
        return tensor.astype(jnp.float32).reshape(row_count, heads_local, -1).transpose(1, 0, 2)

    def gate_terms(pre_act, gap_row, decay_row):
        closing = jax.nn.sigmoid(-to_heads(pre_act)) * gap_row.reshape(heads_local, 1, -1)
        return (closing, jnp.log1p(-closing) + decay_row[:, :, None])

    queries = jax.nn.silu(to_heads(query_pre)) * KD ** (-0.5)
    values = to_heads(input_pre)
    keys_fwd, gate_fwd = gate_terms(forward_pre, forget_gap[0], log_decay[0, 0])
    keys_bwd, gate_bwd = gate_terms(backward_pre, forget_gap[1], log_decay[0, 1])
    identity = (
        jnp.ones((heads_local, KD), jnp.float32),
        jnp.zeros((heads_local, KD, VD), jnp.float32),
    )
    local_fwd, decayed_fwd, offset_fwd, state_fwd = block_pass(queries, keys_fwd, values, gate_fwd)
    incoming_fwd = entering((jnp.exp(offset_fwd), state_fwd), "sp", chain_combine, identity, False)
    forward = local_fwd + jnp.einsum("htd,hde->hte", decayed_fwd, incoming_fwd[1], precision=HIGH)
    local_bwd, decayed_bwd, offset_bwd, state_bwd = block_pass(
        jnp.flip(queries, 1), jnp.flip(keys_bwd, 1), jnp.flip(values, 1), jnp.flip(gate_bwd, 1)
    )
    incoming_bwd = entering((jnp.exp(offset_bwd), state_bwd), "sp", chain_combine, identity, True)
    backward = jnp.flip(
        local_bwd + jnp.einsum("htd,hde->hte", decayed_bwd, incoming_bwd[1], precision=HIGH), 1
    )
    joined = forward + backward
    joined = joined * lax.rsqrt(jnp.mean(joined * joined, axis=-1, keepdims=True) + EPS)
    joined = joined * rec_gain.reshape(heads_local, 1, VD)
    return joined.transpose(1, 0, 2).reshape(row_count, heads_local * VD).astype(jnp.bfloat16)


def convolve(conv_pre, glu_pre, conv_kernel, conv_gain):
    gated = (conv_pre.astype(jnp.float32) * jax.nn.sigmoid(glu_pre.astype(jnp.float32))).astype(
        jnp.bfloat16
    )
    half_width = conv_kernel.shape[0] // 2
    padded = padded_2(gated, (("sp", 0),), half_width)
    convolved = lax.conv_general_dilated(
        padded.astype(jnp.float32)[None],
        conv_kernel.astype(jnp.float32)[:, None, :],
        (1,),
        "VALID",
        dimension_numbers=("NWC", "WIO", "NWC"),
        feature_group_count=gated.shape[1],
        precision=HIGH,
    )[0]
    totals = lax.psum((jnp.sum(convolved, axis=-1), jnp.sum(convolved * convolved, axis=-1)), "tp")
    full_width = convolved.shape[1] * lax.axis_size("tp")
    mean_c = (totals[0] / full_width)[:, None]
    variance = (totals[1] / full_width)[:, None] - mean_c * mean_c
    return jax.nn.silu((convolved - mean_c) * lax.rsqrt(variance + EPS) * conv_gain).astype(
        jnp.bfloat16
    )


def body(
    tokens,
    norm_gain,
    rec_query,
    rec_input,
    rec_forward,
    rec_backward,
    forget_gap,
    log_decay,
    rec_gain,
    conv_value,
    conv_gate,
    conv_kernel,
    conv_gain,
    out_rec,
    out_conv,
):
    row_values = tokens[0].astype(jnp.float32)
    normed = row_values * lax.rsqrt(jnp.mean(row_values * row_values, axis=-1, keepdims=True) + EPS)
    normed = (normed * norm_gain).astype(jnp.bfloat16)
    whole = lax.all_gather(normed, "tp", axis=0, tiled=True)
    row_count = whole.shape[0]
    pieces = (
        lax.all_gather(rec_query, "sp", axis=0, tiled=True),
        lax.all_gather(rec_input, "sp", axis=0, tiled=True),
        lax.all_gather(rec_forward, "sp", axis=0, tiled=True),
        lax.all_gather(rec_backward, "sp", axis=0, tiled=True),
        lax.all_gather(conv_value, "sp", axis=0, tiled=True),
        lax.all_gather(conv_gate, "sp", axis=0, tiled=True),
    )
    results = tuple(
        (
            jnp.dot(whole, weight_piece, preferred_element_type=jnp.float32)
            for weight_piece in pieces
        )
    )
    projected = tuple((result.astype(jnp.bfloat16) for result in results))
    rec_out = recurrence(
        projected[0], projected[1], projected[2], projected[3], forget_gap, log_decay, rec_gain
    )
    conv_out = convolve(projected[4], projected[5], conv_kernel, conv_gain)
    both_out = jnp.concatenate([rec_out, conv_out], axis=1)
    out_local = jnp.concatenate([out_rec, out_conv], axis=0)
    full_columns = lax.all_gather(out_local, "sp", axis=1, tiled=True)
    own_rows = row_count // lax.axis_size("tp")
    rows_part = lax.slice_in_dim(both_out, 0, own_rows * lax.axis_size("tp"), axis=0)
    mixed = lax.psum_scatter(
        jnp.dot(rows_part, full_columns, preferred_element_type=jnp.float32).astype(jnp.bfloat16),
        "tp",
        scatter_dimension=0,
        tiled=True,
    )
    return mixed[None]


MESH = pl.DeviceIdType.MESH
PACK = 8


def dot_as(a, b, ca, cb, precision=HIGH):
    return lax.dot_general(
        a, b, (((ca,), (cb,)), ((), ())), precision=precision, preferred_element_type=jnp.float32
    )


PIECES = (2, 4, 1)
TSUB = 2
LAG = 6
OUTS = 4
OUT_AT = 15
(
    PARAMS, DECAY, _, TOKENS, TOKENS_ON, WEIGHTS, OWN, ACROSS, BESIDE, OUT_OWN, OUT, OUT_ACROSS,
    OUT_BESIDE, GIVE, HALO, STATE, STATS, MIXED, GROUPS,
) = range(19)


def pair_kernel(
    tokens_in, gain_in, w0, w1, w2, w3, w4, w5, decay_in, gap_in, rgain_in, cgain_in, taps_in,
    out_r, out_c, o_ref, decay_v, gap_v, rgain_v, cgain_v, taps_v, tokens, gain,
    xs, x, wbuf, ow, pack, pk, lds, ld, dec, proj, gp, halo_s, halo_r, st_s, st_in, cacc, stat,
    yout, ya, mo, fin, ini, snd, w_own, w_recv, y_recv, d_recv, t_recv, p_recv, l_recv, h_recv,
    s_recv, c_recv, a_recv, o_own, o_recv, q_recv, g_recv, f_recv,
):
    s = lax.axis_index("sp")
    f = lax.axis_index("fs")
    t = lax.axis_index("tp")
    other = 1 - t
    col = lax.rem(f, 2)
    row = f // 2
    part = s // 2
    pair = lax.rem(s, 2)
    near = s + 1 - 2 * pair
    far = lax.rem(s + 2, 4)
    cross = 3 - s
    fx = f + 1 - 2 * col
    fy = lax.rem(f + 2, 4)
    fd = 3 - f
    head = 2 * pair + col
    rows = tokens.shape[1]
    span = 2 * rows
    total = 2 * span
    width = KD
    weights = (w0, w1, w2, w3, w4, w5)
    kslice = w0.shape[0]
    fourth = kslice // 4
    kinds = (range(4, 6), range(1, 4), range(0, 1))
    half = out_r.shape[0]
    quarter = half // 4
    cols = out_r.shape[1]
    groups = 4 * width
    ways = (near, 2 - part, 3 - 3 * part)
    NEAR, INNER, OUTER = range(3)
    mine = OUTER - (pair - part) * (pair - part)
    own_col = t == col
    own_weights = t == pair

    def at(sp=s, fs=f, tp=t):
        return {"sp": sp, "fs": fs, "tp": tp}

    def remote(src, dst, send, recv, to):
        return pltpu.make_async_remote_copy(
            src_ref=src, dst_ref=dst, send_sem=send, recv_sem=recv, device_id=to,
            device_id_type=MESH,
        )

    def when(cond, act):
        if cond is None:
            act()
        else:
            pl.when(cond)(act)

    def send(src, dst, group, recv, to, cond=None):
        when(cond, remote(src, dst, snd.at[group], recv, to).start)

    def arrived(ref, sem, cond=None):
        when(cond, pltpu.make_async_copy(ref, ref, sem).wait)

    def aligned(start, size, unit):
        return pl.ds(pl.multiple_of(start, unit), size)

    entry = [
        pltpu.make_async_copy(src, dst, ini.at[i])
        for i, (src, dst) in enumerate(
            (
                (tokens_in, tokens), (gain_in, gain), (decay_in, decay_v), (gap_in, gap_v),
                (rgain_in, rgain_v), (cgain_in, cgain_v), (taps_in, taps_v),
            )
        )
    ]
    for copy in entry:
        copy.start()

    def slot(place, core, k=None):
        if k is None:
            return aligned(place * span + core * rows, rows, rows)
        step = rows // TSUB
        return aligned(place * span + core * rows + k * step, step, step)

    barrier = pltpu.get_barrier_semaphore()
    greet = [at(sp=lax.rem(s + d, 4), tp=lax.rem(t + c, 2)) for d in range(4) for c in range(2) if d or c]
    greet += [at(sp=z, fs=fx, tp=lax.rem(t + c, 2)) for z in (s, near) for c in range(2)]
    greet += [at(fs=fy), at(fs=fd)]
    for to in greet:
        pl.semaphore_signal(barrier, inc=1, device_id=to, device_id_type=MESH)

    for copy in entry:
        copy.wait()
    values = tokens[0].astype(jnp.float32)
    normed = values * lax.rsqrt(jnp.mean(values * values, axis=-1, keepdims=True) + EPS)
    normed = (normed * gain[...]).astype(jnp.bfloat16)
    xs[...] = normed

    @pl.when(own_col)
    def _():
        x[slot(pair, t), :] = normed

    taps_n = taps_v.shape[0]
    at_col = aligned(col * width, width, width)
    pack[0:2, :] = gap_v[:, at_col]
    pack[2:3, :] = rgain_v[:, at_col]
    pack[3:4, :] = cgain_v[:, at_col]
    pack[4:PACK, :] = jnp.zeros((PACK - 4, width), jnp.float32)
    pack[PACK : PACK + taps_n, :] = taps_v[:, at_col].astype(jnp.float32)
    for j in range(2):
        lds[j, 0:2, :] = decay_v[0, :, j, :]
        lds[j, 2:PACK, :] = jnp.zeros((PACK - 2, span), jnp.float32)
    pl.semaphore_wait(barrier, len(greet))

    def piece(kind, place, side, core, i):
        size = fourth // PIECES[kind]
        at_cols = pl.ds(kinds[kind].start * width, len(kinds[kind]) * width)
        return wbuf.at[
            aligned(place * kslice + (side * 2 + core) * fourth + i * size, size, size), at_cols
        ]

    def flag(kind, way, i):
        return 3 * sum(PIECES[:kind]) + way * PIECES[kind] + i

    def send_weights(kind, i):
        size = fourth // PIECES[kind]
        for place, way in ((far, mine), (cross, mine), (near, NEAR)):
            for core in range(2):
                src_rows = aligned((row * 2 + core) * fourth + i * size, size, size)
                dst_rows = aligned(s * kslice + (row * 2 + core) * fourth + i * size, size, size)
                for m in kinds[kind]:
                    send(
                        weights[m].at[src_rows, at_col],
                        wbuf.at[dst_rows, pl.ds(m * width, width)],
                        WEIGHTS, w_recv.at[flag(kind, way, i)], at(sp=place, tp=core),
                        own_weights if place is far else jnp.logical_not(own_weights),
                    )

    @pl.when(own_weights)
    def _():
        pk[...] = pack[...]

    send(pack, pk, PARAMS, p_recv, at(tp=other), own_weights)
    for j in range(2):
        to = at(sp=2 * part + t, fs=2 * row + j, tp=col)
        here = own_weights & (col == j) & own_col

        @pl.when(here)
        def _(j=j):
            pltpu.make_async_copy(lds.at[j], ld.at[pair], l_recv.at[pair]).start()

        send(lds.at[j], ld.at[pair], DECAY + j, l_recv.at[pair], to, jnp.logical_not(here))

    def send_tokens(k):
        step = rows // TSUB
        src = xs.at[pl.ds(k * step, step)]
        dst = x.at[slot(pair, t, k)]
        sem = t_recv.at[pair, t, k]
        send(src, dst, TOKENS, sem, at(sp=near, tp=col))
        send(src, dst, TOKENS, sem, at(fs=fx, tp=col))
        send(src, dst, TOKENS_ON, sem, at(tp=col), jnp.logical_not(own_col))

    own_rows = aligned(s * kslice, kslice, kslice)
    for m in range(6):

        @pl.when(own_weights)
        def _(m=m):
            src = weights[m].at[:, at_col]
            dst = wbuf.at[own_rows, pl.ds(m * width, width)]
            kind = [m in k for k in kinds].index(True)
            remote(src, dst, snd.at[OWN], w_own.at[kind], at(tp=other)).start()
            pltpu.make_async_copy(src, dst, w_own.at[kind]).start()

    def out_cols(place):
        return aligned(place * cols, cols, cols)

    for which, ref in enumerate((out_r, out_c)):
        dst = ow.at[which, aligned(t * half, half, half), pl.ds(0, cols)]
        pltpu.make_async_copy(ref, dst, o_own.at[0]).start()
        send(ref, dst, OUT_OWN, o_own.at[1], at(tp=other))

    def relay_tokens(k):
        scope(f"T{k}")
        for core in range(2):
            ref = x.at[slot(1 - pair, core, k)]
            arrived(ref, t_recv.at[1 - pair, core, k], own_col)
            send(ref, ref, TOKENS_ON, t_recv.at[1 - pair, core, k], at(fs=fx), own_col)

    def first_hop(kind, way, i):
        scope(f"A{kind}{way}{i}")
        ref = piece(kind, ways[way], row, t, i)
        arrived(ref, w_recv.at[flag(kind, way, i)])
        send(ref, ref, ACROSS, y_recv.at[flag(kind, way, i)], at(fs=fy))
        send(ref, ref, BESIDE, d_recv.at[kind], at(tp=other))

    def second_hop(kind, way, i):
        scope(f"B{kind}{way}{i}")
        ref = piece(kind, ways[way], 1 - row, t, i)
        arrived(ref, y_recv.at[flag(kind, way, i)])
        send(ref, ref, BESIDE, d_recv.at[kind], at(tp=other))

    def weights_wait(kind):
        at_cols = pl.ds(kinds[kind].start * width, len(kinds[kind]) * width)
        arrived(wbuf.at[own_rows, at_cols], w_own.at[kind])
        arrived(wbuf.at[pl.ds(0, 6 * fourth), at_cols], d_recv.at[kind])

    cut = quarter // (OUTS // 2)

    def out_part(core, quart, k):
        return ow.at[
            k // (OUTS // 2),
            aligned(core * half + quart * quarter + k % (OUTS // 2) * cut, cut, cut),
            pl.ds(cols, cols),
        ]

    def send_out(k):
        src = (out_r, out_c)[k // (OUTS // 2)].at[
            aligned(f * quarter + k % (OUTS // 2) * cut, cut, cut), :
        ]
        send(src, out_part(t, f, k), OUT, o_recv.at[k], at(sp=far))

    def out_first(k):
        scope(f"X{k}")
        ref = out_part(t, f, k)
        arrived(ref, o_recv.at[k])
        send(ref, ref, OUT_ACROSS, q_recv.at[k, 0], at(fs=fx))
        send(ref, ref, OUT_ACROSS, q_recv.at[k, 1], at(fs=fy))
        send(ref, ref, OUT_BESIDE, g_recv, at(tp=other))

    def out_second(k):
        scope(f"Y{k}")
        for j, (source, to) in enumerate(((fx, fy), (fy, fx))):
            ref = out_part(t, source, k)
            arrived(ref, q_recv.at[k, j])
            if j == 0:
                send(ref, ref, OUT_ACROSS, q_recv.at[k, 2], at(fs=to))
            send(ref, ref, OUT_BESIDE, g_recv, at(tp=other))

    def out_third(k):
        scope(f"Z{k}")
        ref = out_part(t, fd, k)
        arrived(ref, q_recv.at[k, 2])
        send(ref, ref, OUT_BESIDE, g_recv, at(tp=other))

    def run(step, *pieces):
        for k in pieces:
            step(k)

    def project(kind):
        at_cols = pl.ds(kinds[kind].start * width, len(kinds[kind]) * width)
        proj[:, at_cols] = jnp.dot(
            x[...], wbuf[:, at_cols], preferred_element_type=jnp.float32
        ).astype(jnp.bfloat16)

    for k in range(TSUB):
        send_weights(0, k)
        send_tokens(k)
    for kind in range(1, 3):
        for i in range(PIECES[kind]):
            send_weights(kind, i)
    bf = jnp.bfloat16
    blocks = total // BLOCK
    pad = 16

    def decay_columns():
        scope("dec")
        for place in range(2):
            arrived(ld.at[place], l_recv.at[place])
        arrived(pk, p_recv, jnp.logical_not(own_weights))
        pick = lax.broadcasted_iota(jnp.int32, (PACK, width), 0)
        for place in range(2):
            for d in range(2):
                dec[d, pl.ds(place * span, span), :] = dot_as(
                    ld[place], (pick == d).astype(jnp.float32), 0, 0
                )

    def conv_open():
        scope("tokwait")
        for k in range(TSUB):
            for place in (pair, 1 - pair):
                for core in range(2):
                    local = own_col & (place == pair) & (t == core)
                    done = own_col & (place == 1 - pair)
                    skip = local | done if place is not pair else local
                    arrived(x.at[slot(place, core, k)], t_recv.at[place, core, k], jnp.logical_not(skip))
        scope("cwait")
        weights_wait(0)
        scope("projectc")
        project(0)
        scope("gate")
        conv_pre = proj[:, 4 * width : 5 * width].astype(jnp.float32)
        glu_pre = proj[:, 5 * width : 6 * width].astype(jnp.float32)
        gated = (conv_pre * jax.nn.sigmoid(glu_pre)).astype(jnp.bfloat16)
        gp[pad : pad + total, :] = gated.astype(jnp.float32)
        halo_s[...] = jnp.where(part == 0, gated[total - pad :], gated[0:pad])
        send(halo_s, halo_r, HALO, h_recv, at(sp=far))
        for k in range(OUTS // 2, OUTS):
            send_out(k)

    def conv_close():
        scope("conv")
        arrived(halo_r, h_recv)
        halo = halo_r[...].astype(jnp.float32)
        none = jnp.zeros((pad, width), jnp.float32)
        gp[0:pad, :] = jnp.where(part == 1, halo, none)
        gp[pad + total : 2 * pad + total, :] = jnp.where(part == 0, halo, none)
        first = pad - taps_n // 2
        for b in range(blocks):
            acc = jnp.zeros((BLOCK, width), jnp.float32)
            for j in range(taps_n):
                acc = acc + pk[PACK + j : PACK + j + 1, :] * gp[pl.ds(b * BLOCK + first + j, BLOCK), :]
            cacc[pl.ds(b * BLOCK, BLOCK), :] = acc
        conv = cacc[...]
        ones = jnp.ones((8, width), jnp.float32)
        stat[head, 0] = dot_as(ones, conv, 1, 1)
        stat[head, 1] = dot_as(ones, conv * conv, 1, 1)
        own_stat = stat.at[head]
        send(own_stat, own_stat, STATS, c_recv, at(fs=fx))
        send(own_stat, own_stat, STATS, c_recv, at(sp=near))
        send(own_stat, own_stat, STATS, c_recv, at(sp=near, fs=fx))

    order = [
        (0, INNER, 0), (0, NEAR, 0), (0, INNER, 1), (1, INNER, 0), (0, OUTER, 0), (0, NEAR, 1),
        (1, INNER, 1), (0, OUTER, 1), (1, INNER, 2), (1, OUTER, 0), (1, NEAR, 0), (1, INNER, 3),
        (1, OUTER, 1), (1, NEAR, 1), (1, OUTER, 2), (1, NEAR, 2), (1, OUTER, 3), (1, NEAR, 3),
        (2, INNER, 0), (2, OUTER, 0), (2, NEAR, 0),
    ]
    for k, hop in enumerate(order):
        if k == 4:
            relay_tokens(0)
        if k == 7:
            relay_tokens(1)
        first_hop(*hop)
        if k >= LAG:
            second_hop(*order[k - LAG])
        if k == 5:
            decay_columns()
        if k == OUT_AT:
            for early in range(OUTS // 2):
                send_out(early)
        if k == 17:
            conv_open()
    for hop in order[-LAG:-3]:
        second_hop(*hop)
    scope("kwait")
    weights_wait(1)
    scope("projectk")
    project(1)

    scope("states")
    def f32(n0):
        return proj[:, n0 * width : (n0 + 1) * width].astype(jnp.float32)

    value = proj[:, width : 2 * width]
    keys, gates = [], []
    for d in range(2):
        key = pk[d : d + 1, :] * jax.nn.sigmoid(-f32(2 + d))
        keys.append(key)
        gates.append(jnp.log1p(-key) + dec[d])
    row_i = lax.broadcasted_iota(jnp.int32, (total, total), 0)
    col_i = lax.broadcasted_iota(jnp.int32, (total, total), 1)
    same = (row_i // BLOCK) == (col_i // BLOCK)
    lower = same & (row_i >= col_i)
    upper = same & (row_i <= col_i)
    both = jnp.concatenate(gates, axis=1)
    high = both.astype(bf)
    low = (both - high.astype(jnp.float32)).astype(bf)
    tri = lower.astype(jnp.float32).astype(bf)
    sums = jnp.dot(tri, high, preferred_element_type=jnp.float32) + jnp.dot(
        tri, low, preferred_element_type=jnp.float32
    )
    lasts = [sums[b * BLOCK + BLOCK - 1 : (b + 1) * BLOCK, :] for b in range(blocks)]

    def spread_rows(parts):
        return jnp.concatenate([jnp.broadcast_to(a, (BLOCK, width)) for a in parts], axis=0)

    last = [[a[:, d * width : (d + 1) * width] for a in lasts] for d in range(2)]
    last_rows = [spread_rows(last[d]) for d in range(2)]
    cum_f = sums[:, 0:width]
    cum_b = last_rows[1] - sums[:, width:] + gates[1]
    cums = (cum_f, cum_b)
    key_g = [(keys[d] * jnp.exp(-cums[d])).astype(bf) for d in range(2)]
    weighted = jnp.concatenate(
        [(keys[d] * jnp.exp(last_rows[d] - cums[d])).astype(bf) for d in range(2)], axis=1
    )
    outer = [
        lax.dot_general(
            value[b * BLOCK : (b + 1) * BLOCK], weighted[b * BLOCK : (b + 1) * BLOCK],
            (((0,), (0,)), ((), ())), preferred_element_type=jnp.float32,
        )
        for b in range(blocks)
    ]
    states = [[None] * blocks, [None] * blocks]
    ends, offsets = [], [[None] * blocks, [None] * blocks]
    for d in range(2):
        state = jnp.zeros((width, width), jnp.float32)
        offset = jnp.zeros((1, width), jnp.float32)
        for b in range(blocks) if d == 0 else range(blocks - 1, -1, -1):
            states[d][b] = state
            offsets[d][b] = offset
            state = state * jnp.exp(last[d][b]) + outer[b][:, d * width : (d + 1) * width]
            offset = offset + last[d][b]
        ends.append(state)
    st_s[...] = jnp.where(part == 0, ends[0], ends[1]).astype(bf)
    send(st_s, st_in, STATE, s_recv, at(sp=far))


    for hop in order[-3:]:
        second_hop(*hop)
    run(out_first, 0, 1)
    conv_close()
    scope("qwait")
    weights_wait(2)
    scope("projectq")
    project(2)
    scope("scores")
    query_pre = f32(0)
    query = query_pre * jax.nn.sigmoid(query_pre) * width ** (-0.5)
    query_g = [(query * jnp.exp(cums[d])).astype(bf) for d in range(2)]
    scores = [
        lax.dot_general(
            query_g[d], key_g[d], (((1,), (1,)), ((), ())), preferred_element_type=jnp.float32
        )
        for d in range(2)
    ]
    scores = (jnp.where(lower, scores[0], 0.0) + jnp.where(upper, scores[1], 0.0)).astype(bf)
    inner = jnp.dot(scores, value, preferred_element_type=jnp.float32)
    carried = jnp.concatenate(
        [
            lax.dot_general(
                jnp.concatenate([q[b * BLOCK : (b + 1) * BLOCK] for q in query_g], axis=1),
                jnp.concatenate([states[d][b].astype(bf) for d in range(2)], axis=1),
                (((1,), (1,)), ((), ())), preferred_element_type=jnp.float32,
            )
            for b in range(blocks)
        ],
        axis=0,
    )
    reach = jnp.where(
        part == 1, spread_rows(offsets[0]) + cum_f, spread_rows(offsets[1]) + cum_b
    )
    query_in = (query * jnp.exp(reach)).astype(bf)
    def mix(which, out):
        for core in range(2):
            for place in range(2):
                at_row = place * span + core * rows
                yout[which, pl.ds(core * span + place * rows, rows), :] = out[
                    at_row : at_row + rows
                ].astype(bf)
        dst = ya.at[:, aligned(which * groups + head * width, width, width)]
        for place in (near, s):
            for core in range(2):
                src = yout.at[which, pl.ds(core * span, span)]
                here = own_col & (place == s) & (t == core)

                @pl.when(here)
                def _(src=src):
                    pltpu.make_async_copy(src, dst, a_recv.at[which]).start()

                send(
                    src, dst, MIXED, a_recv.at[which],
                    at(sp=place, fs=2 * row + t, tp=core), jnp.logical_not(here),
                )

    run(out_first, 2, 3)
    scope("statein")
    arrived(st_in, s_recv)
    scope("recnorm")
    joined = inner + carried + lax.dot_general(
        query_in, st_in[...], (((1,), (1,)), ((), ())), preferred_element_type=jnp.float32
    )
    joined = joined * lax.rsqrt(jnp.mean(joined * joined, axis=-1, keepdims=True) + EPS)
    mix(0, joined * pk[2:3, :])

    run(out_second, 0, 1)
    scope("statx")
    arrived(stat.at[pl.ds(0, 3)], c_recv)
    scope("cnorm")
    stats = (stat[0] + stat[1] + stat[2] + stat[3]) / groups
    mean_r = stats[0]
    inv_r = lax.rsqrt(stats[1] - mean_r * mean_r + EPS)
    eighth = jnp.full((8, width), 0.125, jnp.float32)
    mean_c = dot_as(mean_r, eighth, 0, 0)
    inv_c = dot_as(inv_r, eighth, 0, 0)
    out = (cacc[...] - mean_c) * inv_c * pk[3:4, :]
    mix(1, out * jax.nn.sigmoid(out))

    run(out_second, 2, 3)
    run(out_third, 0, 1, 2, 3)
    scope("ywait1")
    arrived(ya.at[:, pl.ds(0, groups)], a_recv.at[1])
    for k in range(2):
        arrived(ow.at[:, pl.ds(0, half), pl.ds(0, cols)], o_own.at[k])
    scope("ywait0")
    arrived(ya.at[:, pl.ds(0, groups)], a_recv.at[0])
    near_rows = aligned((1 - pair) * rows, rows, rows)
    own_rows = aligned(pair * rows, rows, rows)

    def product(at_rows, k):
        at_n = pl.ds(k * cols, cols)
        acc = jnp.dot(ya[at_rows, 0:groups], ow[0, :, at_n], preferred_element_type=jnp.float32)
        acc = acc + jnp.dot(ya[at_rows, groups:], ow[1, :, at_n], preferred_element_type=jnp.float32)
        return acc.astype(bf)

    for k in range(2):
        if k == 1:
            arrived(ow.at[:, pl.ds(0, half), pl.ds(0, cols)], g_recv)
        at_n = pl.ds(k * cols, cols)
        mo[near_rows, at_n] = product(near_rows, k)
        send(mo.at[near_rows, at_n], fin.at[:, at_n], GIVE, f_recv.at[k], at(sp=near))
    for k, place in enumerate((s, far)):
        o_ref[0, :, out_cols(place)] = product(own_rows, k)
    for k, place in enumerate((near, cross)):
        scope(f"give{k}")
        at_n = pl.ds(k * cols, cols)
        arrived(fin.at[:, at_n], f_recv.at[k])
        o_ref[0, :, out_cols(place)] = fin[:, at_n]

    scope("sendwaits")
    other_weights = jnp.logical_not(own_weights)
    other_col = jnp.logical_not(own_col)
    arrived(pack, snd.at[PARAMS], own_weights)
    for j in range(2):
        here = own_weights & (col == j) & own_col
        arrived(lds.at[j], snd.at[DECAY + j], jnp.logical_not(here))
    arrived(x.at[pl.ds(0, 2 * rows)], snd.at[TOKENS])
    arrived(x.at[pl.ds(0, 2 * rows)], snd.at[TOKENS_ON], own_col)
    arrived(x.at[pl.ds(0, rows)], snd.at[TOKENS_ON], other_col)
    arrived(wbuf.at[pl.ds(0, 2 * fourth)], snd.at[WEIGHTS], own_weights)
    arrived(wbuf.at[pl.ds(0, 4 * fourth)], snd.at[WEIGHTS], other_weights)
    arrived(wbuf.at[pl.ds(0, kslice)], snd.at[OWN], own_weights)
    arrived(wbuf.at[pl.ds(0, 3 * fourth)], snd.at[ACROSS])
    arrived(wbuf.at[pl.ds(0, 6 * fourth)], snd.at[BESIDE])
    arrived(ow.at[:, pl.ds(0, half), pl.ds(0, cols)], snd.at[OUT_OWN])
    arrived(ow.at[:, pl.ds(0, quarter), pl.ds(0, cols)], snd.at[OUT])
    arrived(ow.at[:, pl.ds(0, 3 * quarter), pl.ds(0, cols)], snd.at[OUT_ACROSS])
    arrived(ow.at[:, pl.ds(0, 4 * quarter), pl.ds(0, cols)], snd.at[OUT_BESIDE])
    arrived(halo_s, snd.at[HALO])
    arrived(st_s, snd.at[STATE])
    arrived(stat.at[pl.ds(0, 3)], snd.at[STATS])
    arrived(x.at[pl.ds(0, 6 * span * width // x.shape[1])], snd.at[MIXED], own_col)
    arrived(x.at[pl.ds(0, 8 * span * width // x.shape[1])], snd.at[MIXED], other_col)
    arrived(fin, snd.at[GIVE])
    scope(None)


def scope(name):
    pass


def pair_body(
    tokens, norm_gain, rec_query, rec_input, rec_forward, rec_backward, forget_gap,
    log_decay, rec_gain, conv_value, conv_gate, conv_kernel, conv_gain, out_rec, out_conv,
):
    rows, d = tokens.shape[1:]
    total = 4 * rows
    taps = conv_kernel.shape[0]
    width = KD
    half, cols = out_rec.shape

    bf, f32 = jnp.bfloat16, jnp.float32
    dma = pltpu.SemaphoreType.DMA
    small = (log_decay, forget_gap, rec_gain[None], conv_gain[None], conv_kernel)
    scratch = [
        *(pltpu.VMEM(a.shape, a.dtype) for a in small),
        pltpu.VMEM(tokens.shape, bf),
        pltpu.VMEM((1, d), f32),
        pltpu.VMEM((rows, d), bf),
        pltpu.VMEM((total, d), bf),
        pltpu.VMEM((d, 6 * width), bf),
        pltpu.VMEM((2, 2 * half, 2 * cols), bf),
        pltpu.VMEM((PACK + taps, width), f32),
        pltpu.VMEM((PACK + taps, width), f32),
        pltpu.VMEM((2, PACK, 2 * rows), f32),
        pltpu.VMEM((2, PACK, 2 * rows), f32),
        pltpu.VMEM((2, total, width), f32),
        pltpu.VMEM((total, 6 * width), bf),
        pltpu.VMEM((total + 32, width), f32),
        pltpu.VMEM((16, width), bf),
        pltpu.VMEM((16, width), bf),
        pltpu.VMEM((width, width), bf),
        pltpu.VMEM((width, width), bf),
        pltpu.VMEM((total, width), f32),
        pltpu.VMEM((4, 2, 8, total), f32),
        pltpu.VMEM((2, total, width), bf),
        pltpu.VMEM((2 * rows, 8 * width), bf),
        pltpu.VMEM((2 * rows, 2 * cols), bf),
        pltpu.VMEM((rows, 2 * cols), bf),
        dma((7,)), dma((GROUPS,)), dma((3,)), dma((3 * sum(PIECES),)), dma((3 * sum(PIECES),)),
        dma((3,)), dma((2, 2, TSUB)), dma(()), dma((2,)), dma(()),
        dma(()), dma(()), dma((2,)), dma((2,)), dma((OUTS,)), dma((OUTS, 3)), dma(()), dma((2,)),
    ]
    return pl.pallas_call(
        pair_kernel,
        out_shape=pltpu.VMEM((1, rows, d), bf),
        in_specs=[pl.BlockSpec(memory_space=pl.ANY)] * 15,
        out_specs=pl.BlockSpec(memory_space=pltpu.VMEM),
        scratch_shapes=scratch,
        compiler_params=pltpu.CompilerParams(
            collective_id=0, has_side_effects=True, vmem_limit_bytes=60 * 1024 * 1024
        ),
    )(
        tokens, norm_gain[None], rec_query, rec_input, rec_forward, rec_backward, conv_value,
        conv_gate, *small, out_rec, out_conv,
    )


def fits(n, nf, nt, tokens, rec_query, log_decay, conv_value, conv_kernel, out_rec):
    heads = log_decay.shape[2]
    rows = tokens.shape[1] // (n * nt)
    return (
        nt == 2
        and n == 4
        and nf == 4
        and n == heads
        and tokens.shape[0] == nf
        and rec_query.shape[1] == heads * KD
        and conv_value.shape[1] == heads * VD
        and KD == VD
        and 2 * rows == KD
        and rows % (16 * TSUB) == 0
        and rec_query.shape[0] % (n * 4 * max(PIECES) * 16) == 0
        and out_rec.shape[0] % (nt * nf * 16) == 0
        and conv_kernel.shape[0] // 2 <= 15
    )


def layer(mesh, *args):
    n, nf, nt = (mesh.shape[a] for a in ("sp", "fs", "tp"))
    fast = fits(n, nf, nt, args[0], args[2], args[7], args[9], args[11], args[13])
    return sharded(mesh, pair_body if fast else body)(*args)


def solution(mesh):
    return functools.partial(layer, mesh)


def sharded(mesh, body):
    return jax.shard_map(
        body,
        mesh=mesh,
        in_specs=(
            P("fs", ("sp", "tp"), None),
            P(),
            P("sp", "tp"),
            P("sp", "tp"),
            P("sp", "tp"),
            P("sp", "tp"),
            P(None, "tp"),
            P("fs", None, "tp", "sp"),
            P("tp"),
            P("sp", "tp"),
            P("sp", "tp"),
            P(None, "tp"),
            P("tp"),
            P("tp", "sp"),
            P("tp", "sp"),
        ),
        out_specs=P("fs", ("sp", "tp"), None),
        check_vma=False,
    )
```
